256 devices in a mesh: sp: 32 (over z, x), tp: 8 (over y, core).
Axes of the slice: x: 4, y: 4, z: 8, core: 2. Of those that a mesh axis runs over, the one named last changes fastest.
Arguments:
- query_rows: bfloat16 [32768, 1024], P('sp', 'tp'), may hold values from -8 to 8
- key_rows: bfloat16 [32768, 1024], P('sp', 'tp'), may hold values from -8 to 8
- value_rows: bfloat16 [32768, 1024], P('sp', 'tp'), may hold values from -6 to 6
- forget_cum: float32 [16, 32768], P('tp', 'sp'), may hold values from -32768 to 0, as said below
- doc_ids: int32 [32768], P('sp'), may hold values from 0 to 15, never falling along the last dimension, each value on 1 to 3072 neighbouring positions
- residual: bfloat16 [32768, 2048], P(('sp', 'tp')), may hold values from -6 to 6
- out_weight: bfloat16 [1024, 2048], replicated, may hold values from -1.5 to 1.5
- norm_gain: float32 [2048], replicated, may hold values from 0.1 to 1.9
- expert_ids: int32 [32768, 2], P(('sp', 'tp')), may hold values from 0 to 31, as said below
- route_weights: float32 [32768, 2], P(('sp', 'tp')), may hold values from 0.2 to 1
- gate_proj: bfloat16 [32, 2048, 512], P('sp'), may hold values from -0.125 to 0.125
- up_proj: bfloat16 [32, 2048, 512], P('sp'), may hold values from -0.125 to 0.125
- down_proj: bfloat16 [32, 512, 2048], P('sp'), may hold values from -0.25 to 0.25
Outputs:
- layer_out: bfloat16 [32768, 2048], P(('sp', 'tp'))
The draws below stay inside these ranges and needn't reach their ends.
Inputs may be any that keep to these rules, and one draw needn't show every extreme that they name: `forget_cum`: each head's values never rise along the positions. `doc_ids`: document numbers never fall along the positions; a document holds at most 3072 positions, and one holds exactly 3072. `expert_ids`: a token's 2 experts differ and lie in one group of 4 consecutive experts; among the 128 rows of one device no expert is named more than 20 times, and in every draw one expert is named exactly 20 times by the rows of every device.
All inputs are finite; a program needn't handle non-finite values.
Results may differ from the reference program's by a relative error of at most 0.0054.
Values may be sent and summed in bfloat16 or wider, within the bound.
A program may use at most 128 MiB of HBM per device.

```python
import math
import jax
import jax.numpy as jnp
import numpy as np
from jax import lax

D = 2048
HEAD_COUNT = 16
HD = 64
FFE = 512
EPG = 4
TOPK = 2
REACH = 3
TOK_DEV = 1024
TOKEN_COUNT = 32768
TOK_LOC = 128
MOST = 3072
DOCS = 16
EXPERTS = 32
GROUPS = 8
CAP = 20


def draw_query_rows(key, part):
    width = HEAD_COUNT * HD
    base = jnp.clip(jax.random.normal(jax.random.fold_in(key, 1), (TOKEN_COUNT, width), jnp.float32), -6.0, 6.0)
    return base.astype(jnp.bfloat16)


def draw_key_rows(key, part):
    width = HEAD_COUNT * HD
    base = jnp.clip(jax.random.normal(jax.random.fold_in(key, 3), (TOKEN_COUNT, width), jnp.float32), -6.0, 6.0)
    return base.astype(jnp.bfloat16)


def draw_forget_cum(key, part):
    order = jax.random.permutation(jax.random.fold_in(key, 5), HEAD_COUNT)
    fast_count = HEAD_COUNT // 2
    quick_route = order < fast_count
    fast_rate = jnp.exp(jax.random.uniform(jax.random.fold_in(key, 6), (HEAD_COUNT,), jnp.float32, jnp.log(1.0 / 100.0), jnp.log(1.0 / 30.0)))
    slow_rate = jnp.exp(jax.random.uniform(jax.random.fold_in(key, 7), (HEAD_COUNT,), jnp.float32, jnp.log(0.3), jnp.log(1.0))) / TOKEN_COUNT
    rate = jnp.where(quick_route, fast_rate, slow_rate)
    device_factor = jnp.exp(jax.random.uniform(jax.random.fold_in(key, 8), (HEAD_COUNT, TOKEN_COUNT // TOK_DEV), jnp.float32, jnp.log(0.5), jnp.log(2.0)))
    device_factor = jnp.repeat(device_factor, TOK_DEV, axis=1)
    rough = jax.random.uniform(jax.random.fold_in(key, 9), (HEAD_COUNT, TOKEN_COUNT), jnp.float32, 0.0, 2.0)
    gate_logarithm = -rate[:, None] * device_factor * rough
    spike_positions = jax.random.randint(jax.random.fold_in(key, 10), (HEAD_COUNT, 2), 0, TOKEN_COUNT)
    spike_loss = jax.random.uniform(jax.random.fold_in(key, 11), (HEAD_COUNT, 2), jnp.float32, jnp.log(0.5), jnp.log(0.8))
    target_locations = jnp.arange(TOKEN_COUNT, dtype=jnp.int32)
    match_counts = target_locations[None, None, :] == spike_positions[:, :, None]
    spike_events = jnp.sum(jnp.where(match_counts, spike_loss[:, :, None], 0.0), axis=1)
    gate_logarithm = gate_logarithm + jnp.where(quick_route[:, None], 0.0, spike_events)
    return jnp.cumsum(gate_logarithm, axis=1).astype(jnp.float32)


def draw_expert_ids(key, part):
    block_total = TOKEN_COUNT // TOK_LOC
    busy_group = jax.random.randint(jax.random.fold_in(key, 12), (), 0, GROUPS)
    busy_local = jax.random.randint(jax.random.fold_in(key, 13), (), 0, EPG)

    def one_block(block_key):
        others = jnp.arange((GROUPS - 1) * CAP, dtype=jnp.int32) // CAP
        others = others + (others >= busy_group).astype(jnp.int32)
        chosen = jax.random.permutation(jax.random.fold_in(block_key, 1), others)[:TOK_LOC - CAP]
        groups = jnp.concatenate([jnp.full((CAP,), busy_group, jnp.int32), chosen.astype(jnp.int32)])
        groups = jax.random.permutation(jax.random.fold_in(block_key, 2), groups)
        first = jax.random.randint(jax.random.fold_in(block_key, 3), (TOK_LOC,), 0, EPG)
        first = jnp.where(groups == busy_group, busy_local, first)
        second = (first + jax.random.randint(jax.random.fold_in(block_key, 4), (TOK_LOC,), 1, EPG)) % EPG
        swap = jax.random.randint(jax.random.fold_in(block_key, 5), (TOK_LOC,), 0, 2)
        lower = jnp.where(swap == 1, second, first)
        upper = jnp.where(swap == 1, first, second)
        return jnp.stack([groups * EPG + lower, groups * EPG + upper], axis=1).astype(jnp.int32)
    block_keys = jax.random.split(jax.random.fold_in(key, 14), block_total)
    return jax.vmap(one_block)(block_keys).reshape(TOKEN_COUNT, TOPK).astype(jnp.int32)


def shard_levels(stream_key, shape, cuts, least, largest):
    def one(position, blocks):
        draws = jax.random.uniform(jax.random.fold_in(jax.random.fold_in(stream_key, 6), position), (blocks,), jnp.float32, least / len(cuts), largest / len(cuts))
        return jnp.repeat(jnp.exp(draws), shape[position] // blocks).reshape((-1,) + (1,) * (len(shape) - position - 1))

    gain = one(*cuts[0])
    for cut in cuts[1:]:
        gain = gain * one(*cut)
    return gain


def split_up(amount, total, reach, slope):
    loads = [(1 << 20) // math.isqrt(standing ** slope) + 1 for standing in range(2, amount + 1)]
    rest, given = total - reach - (amount - 1), [1] * (amount - 1)
    while rest > 0:
        candidates = [i for i in range(amount - 1) if given[i] < reach]
        mass, left = sum([loads[i] for i in candidates]), rest
        for i in candidates:
            addition = min(reach - given[i], max(1, left * loads[i] // mass), rest)
            given[i] = given[i] + addition
            rest = rest - addition
    return np.array([reach] + given)


def ragged(key, count, total, limit, slope):
    if count == 2:
        one = jax.random.randint(key, (), max(1, total - limit), min(limit, total - 1) + 1)
        return jnp.stack([one, total - one])
    tallies = jnp.asarray(split_up(count, total, limit, slope), jnp.int32)
    pairs = (count - 1) // 2
    source_of, taker = tallies[1:1 + 2 * pairs:2], tallies[2:2 + 2 * pairs:2]
    slack = jnp.minimum(source_of - 1, limit - taker)
    moved = jax.random.randint(jax.random.fold_in(key, 1), (pairs,), 0, 1 << 20) % (slack + 1)
    tallies = tallies.at[1:1 + 2 * pairs:2].set(source_of - moved).at[2:2 + 2 * pairs:2].set(taker + moved)
    return tallies[jax.random.permutation(jax.random.fold_in(key, 2), count)]


def bell_draw(rng, shape, deviation, bound, pieces=(), kind=jnp.bfloat16):
    drawn = jax.random.normal(rng, shape, jnp.float32) * deviation
    if len(pieces) > 0:
        drawn = shard_levels(rng, shape, pieces, -0.22, 0.18) * drawn
    return jnp.clip(drawn, min=-bound, max=bound).astype(kind)


def setup_inputs(seed: int = 0) -> dict:
    key_of = jax.random.split(jax.random.key(seed), 14)
    query_rows = draw_query_rows(jax.random.fold_in(key_of[13], 71), 0)
    key_rows = draw_key_rows(jax.random.fold_in(key_of[13], 71), 0)
    value_rows = bell_draw(key_of[2], (TOKEN_COUNT, HEAD_COUNT * HD), 1.0, 6.0, ((0, 32), (1, 8)))
    forget_cum = draw_forget_cum(jax.random.fold_in(key_of[13], 71), 0)
    doc_ids = jnp.searchsorted(jnp.cumsum(ragged(key_of[4], DOCS, TOKEN_COUNT, MOST, 2)), jnp.arange(TOKEN_COUNT), side="right").astype(jnp.int32)
    residual = bell_draw(key_of[5], (TOKEN_COUNT, D), 1.0, 6.0, ((0, 256),))
    out_weight = bell_draw(key_of[6], (HEAD_COUNT * HD, D), HEAD_COUNT ** -0.5, 1.5)
    norm_gain = jnp.clip(1.0 + 0.18 * jax.random.normal(key_of[7], (D,), jnp.float32), 0.1, 1.9)
    expert_ids = draw_expert_ids(jax.random.fold_in(key_of[13], 71), 0)
    route_weights = jnp.clip(0.2 + 0.8 * jax.random.uniform(key_of[9], (TOKEN_COUNT, TOPK), jnp.float32) ** shard_levels(key_of[9], (TOKEN_COUNT, TOPK), ((0, 256),), -0.2, 0.2), 0.2, 1.0)
    gate_proj = bell_draw(key_of[10], (EXPERTS, D, FFE), D ** -0.5, 0.125, ((0, 32),))
    up_proj = bell_draw(key_of[11], (EXPERTS, D, FFE), D ** -0.5, 0.125, ((0, 32),))
    down_proj = bell_draw(key_of[12], (EXPERTS, FFE, D), FFE ** -0.5, 0.25, ((0, 32),))
    return dict(query_rows=query_rows, key_rows=key_rows, value_rows=value_rows, forget_cum=forget_cum, doc_ids=doc_ids, residual=residual, out_weight=out_weight, norm_gain=norm_gain, expert_ids=expert_ids, route_weights=route_weights, gate_proj=gate_proj, up_proj=up_proj, down_proj=down_proj)


norm_eps = 1e-06
row_block = 128

def attention(query_rows, key_rows, value_rows, forget_cum, doc_ids):
    width = HEAD_COUNT * HD
    back = REACH * TOK_DEV
    span = back + TOK_DEV
    keys_pad = jnp.concatenate([jnp.zeros((back, width), jnp.bfloat16), key_rows], axis=0)
    values_pad = jnp.concatenate([jnp.zeros((back, width), jnp.bfloat16), value_rows], axis=0)
    gates_pad = jnp.concatenate([jnp.zeros((HEAD_COUNT, back), jnp.float32), forget_cum], axis=1)
    docs_pad = jnp.concatenate([jnp.full((back,), -1, jnp.int32), doc_ids.astype(jnp.int32)], axis=0)
    scale = HD ** (-0.5)

    def attend_block(index):
        start = (index * TOK_DEV).astype(jnp.int32)
        query = lax.dynamic_slice_in_dim(query_rows, start, TOK_DEV, 0).reshape(TOK_DEV, HEAD_COUNT, HD).astype(jnp.float32)
        keys = lax.dynamic_slice_in_dim(keys_pad, start, span, 0).reshape(span, HEAD_COUNT, HD).astype(jnp.float32)
        values = lax.dynamic_slice_in_dim(values_pad, start, span, 0).reshape(span, HEAD_COUNT, HD).astype(jnp.float32)
        query_gate = lax.dynamic_slice_in_dim(forget_cum, start, TOK_DEV, 1)
        key_gate = lax.dynamic_slice_in_dim(gates_pad, start, span, 1)
        query_doc = lax.dynamic_slice_in_dim(doc_ids.astype(jnp.int32), start, TOK_DEV, 0)
        key_doc = lax.dynamic_slice_in_dim(docs_pad, start, span, 0)
        score = jnp.einsum('thd,uhd->htu', query, keys) * scale
        score = score + query_gate[:, :, None] - key_gate[:, None, :]
        query_pos = start + jnp.arange(TOK_DEV, dtype=jnp.int32)
        key_pos = start - back + jnp.arange(span, dtype=jnp.int32)
        allowed = (key_pos[None, :] <= query_pos[:, None]) & (key_doc[None, :] == query_doc[:, None])
        score = jnp.where(allowed[None], score, -jnp.inf)
        top = lax.optimization_barrier(jnp.max(score, axis=-1))
        expo = jnp.exp(score - top[..., None])
        total = lax.optimization_barrier(jnp.sum(expo, axis=-1))
        rounded = lax.optimization_barrier(expo.astype(jnp.bfloat16)).astype(jnp.float32)
        summed = jnp.einsum('htu,uhd->thd', rounded, values)
        result = summed / jnp.transpose(total)[:, :, None]
        return result.astype(jnp.bfloat16).reshape(TOK_DEV, width)
    blocks = lax.map(attend_block, jnp.arange(TOKEN_COUNT // TOK_DEV, dtype=jnp.int32))
    return blocks.reshape(TOKEN_COUNT, width)

def experts_layer(normed, expert_ids, route_weights, gate_proj, up_proj, down_proj):
    assign = TOKEN_COUNT * TOPK
    flat_expert = expert_ids.reshape(assign).astype(jnp.int32)
    flat_token = (jnp.arange(assign, dtype=jnp.int32) // TOPK).astype(jnp.int32)
    flat_weight = route_weights.reshape(assign)
    order = jnp.argsort(flat_expert, stable=True)
    sorted_expert = flat_expert[order]
    sorted_token = flat_token[order]
    sorted_weight = flat_weight[order]
    counts = jnp.bincount(flat_expert, length=EXPERTS).astype(jnp.int32)
    padded = (counts + row_block - 1) // row_block * row_block
    start = jnp.cumsum(counts) - counts
    pad_end = jnp.cumsum(padded)
    pad_start = pad_end - padded
    dest = (pad_start[sorted_expert] + jnp.arange(assign, dtype=jnp.int32) - start[sorted_expert]).astype(jnp.int32)
    block_count = (assign + EXPERTS * (row_block - 1) + row_block - 1) // row_block
    buffer = jnp.zeros((block_count * row_block, D), jnp.bfloat16).at[dest].set(normed[sorted_token])
    block_expert = jnp.clip(jnp.searchsorted(pad_end, jnp.arange(block_count, dtype=jnp.int32) * row_block, side='right'), 0, EXPERTS - 1).astype(jnp.int32)

    def run_block(args):
        rows, expert = args
        gate = jnp.dot(rows, gate_proj[expert], preferred_element_type=jnp.float32)
        up = jnp.dot(rows, up_proj[expert], preferred_element_type=jnp.float32)
        act = (jax.nn.silu(gate) * up).astype(jnp.bfloat16)
        return jnp.dot(act, down_proj[expert], preferred_element_type=jnp.float32).astype(jnp.bfloat16)
    results = lax.map(run_block, (buffer.reshape(block_count, row_block, D), block_expert)).reshape(-1, D)
    contrib = results[dest].astype(jnp.float32) * sorted_weight[:, None]
    return jnp.zeros((TOKEN_COUNT, D), jnp.float32).at[sorted_token].add(contrib)

def reference(query_rows, key_rows, value_rows, forget_cum, doc_ids, residual, out_weight, norm_gain, expert_ids, route_weights, gate_proj, up_proj, down_proj):
    attended = attention(query_rows, key_rows, value_rows, forget_cum, doc_ids)
    mixed = jnp.dot(attended, out_weight, preferred_element_type=jnp.float32)
    hidden = residual.astype(jnp.float32) + mixed
    normed = (hidden * lax.rsqrt(lax.optimization_barrier(jnp.mean(hidden * hidden, axis=-1, keepdims=True)) + norm_eps) * norm_gain).astype(jnp.bfloat16)
    routed = experts_layer(normed, expert_ids, route_weights, gate_proj, up_proj, down_proj)
    return (hidden + routed).astype(jnp.bfloat16)
```

```python
import functools
import jax
import jax.numpy as jnp
from jax import lax
from jax.experimental import pallas as pl
from jax.experimental.pallas import tpu as pltpu
from jax.sharding import PartitionSpec as P

EPG = 4
TOPK = 2
REACH = 3
QT = 256
KT = 512
FAR = -1e30

norm_eps = 1e-06
F32 = jnp.float32
BF16 = jnp.bfloat16


def columns_of(rows):
    parts = [jnp.transpose(rows[:, c : c + 128]) for c in range(0, rows.shape[1], 128)]
    return jnp.concatenate(parts, axis=0).astype(BF16)


def mixer_kernel(
    n_sp, n_tp, q_ref, k_ref, v_ref, marks_ref, out_ref,
    kbuf, vbuf, mbuf, qaug, kmark, vaug, top, acc, att, heads,
    ksend, krecv, vsend, vrecv, msend, mrecv, hsend, hrecv,
):
    sp = lax.axis_index("sp")
    tp = lax.axis_index("tp")
    tok = q_ref.shape[0]
    chunk = tok // n_tp

    barrier = pltpu.get_barrier_semaphore()
    for d in range(1, REACH + 1):
        for other in (lax.rem(sp + d, n_sp), lax.rem(sp + n_sp - d, n_sp)):
            pl.semaphore_signal(barrier, inc=1, device_id={"sp": other})
    for d in range(1, n_tp):
        pl.semaphore_signal(barrier, inc=1, device_id={"tp": lax.rem(tp + d, n_tp)})
    pl.semaphore_wait(barrier, 2 * REACH + n_tp - 1)

    halo = []
    for d in range(1, REACH + 1):
        ahead = {"sp": lax.rem(sp + d, n_sp)}
        parts = []
        for src, buf, send, recv in (
            (marks_ref, mbuf, msend, mrecv), (k_ref, kbuf, ksend, krecv), (v_ref, vbuf, vsend, vrecv)
        ):
            copy = pltpu.make_async_remote_copy(
                src_ref=src, dst_ref=buf.at[d - 1], send_sem=send.at[d - 1], recv_sem=recv.at[d - 1],
                device_id=ahead,
            )
            copy.start()
            parts.append(copy)
        halo.append(parts)

    lane = lax.broadcasted_iota(jnp.int32, (1, 128), 1)
    row8 = lax.broadcasted_iota(jnp.int32, (8, tok), 0)
    row16 = lax.broadcasted_iota(jnp.int32, (16, tok), 0).astype(F32)
    blank = jnp.zeros((104, tok), F32)
    own = marks_ref[...]
    base = own[0:2, 0:1]

    same = (own[2:3, :] == row16).astype(F32)
    qmark = columns_of(jnp.concatenate([jnp.zeros((8, tok), F32), same, blank], axis=0))
    qrows = q_ref[...] * jnp.asarray(0.125, BF16)
    for h in range(2):
        mine = (lane >= 64 * h) & (lane < 64 * h + 64)
        ones = (lane >= 3 * h) & (lane < 3 * h + 3)
        qaug[h, :, 0:128] = jnp.where(mine, qrows, jnp.zeros_like(qrows))
        qaug[h, :, 128:256] = jnp.where(ones, jnp.ones_like(qmark), qmark)

    def prepare(marks, v):
        gate = base - marks[0:2, :]
        high = gate.astype(BF16).astype(F32)
        rest = gate - high
        mid = rest.astype(BF16).astype(F32)
        low = rest - mid
        pieces = jnp.zeros((8, tok), F32)
        for h in range(2):
            for i, piece in enumerate((high, mid, low)):
                pieces = jnp.where(row8 == 3 * h + i, piece[h : h + 1, :], pieces)
        other = jnp.where(marks[2:3, :] == row16, 0.0, FAR).astype(F32)
        kmark[...] = columns_of(jnp.concatenate([pieces, other, blank], axis=0))
        one = jnp.ones_like(v)
        vaug[0] = jnp.where(lane < 64, v, one)
        vaug[1] = jnp.where(lane < 64, one, v)

    def tile(keys, q0, k0, fresh, causal):
        rows = pl.ds(q0, QT)
        kk = jnp.concatenate([keys[pl.ds(k0, KT), :], kmark[pl.ds(k0, KT), :]], axis=1)
        for h in range(2):
            score = lax.dot_general(
                qaug[h, rows, :], kk, (((1,), (1,)), ((), ())), preferred_element_type=F32
            )
            if causal:
                qpos = q0 + lax.broadcasted_iota(jnp.int32, (QT, KT), 0)
                kpos = k0 + lax.broadcasted_iota(jnp.int32, (QT, KT), 1)
                score = jnp.where(kpos <= qpos, score, FAR)
            best = jnp.broadcast_to(jnp.max(score, axis=1, keepdims=True), (QT, 128))
            if not fresh:
                old = top[h, rows, :]
                best = jnp.maximum(best, old)
            expo = jnp.exp(score - jnp.concatenate([best] * (KT // 128), axis=1)).astype(BF16)
            part = jnp.dot(expo, vaug[h, pl.ds(k0, KT), :], preferred_element_type=F32)
            if not fresh:
                part = acc[h, rows, :] * jnp.exp(old - best) + part
            top[h, rows, :] = best
            acc[h, rows, :] = part

    prepare(own, v_ref[...])
    tiles = tok // QT
    per = KT // QT
    for k0 in range(0, tok, KT):
        first = k0 // QT

        def diagonal(i, carry, k0=k0):
            tile(k_ref, pl.multiple_of(i * QT, QT), k0, k0 == 0, True)
            return carry

        def below(i, carry, k0=k0):
            tile(k_ref, pl.multiple_of(i * QT, QT), k0, k0 == 0, False)
            return carry

        lax.fori_loop(first, first + per, diagonal, 0)
        if first + per < tiles:
            lax.fori_loop(first + per, tiles, below, 0)

    for d in range(1, REACH + 1):
        for copy in halo[d - 1]:
            copy.wait_recv()
        prepare(mbuf[d - 1], vbuf[d - 1])
        keys = kbuf.at[d - 1]
        if d < REACH:

            def full(i, carry, keys=keys):
                for k0 in range(0, tok, KT):
                    tile(keys, pl.multiple_of(i * QT, QT), k0, False, False)
                return carry

            lax.fori_loop(0, tiles, full, 0)

    keys = kbuf.at[REACH - 1]
    sends = []
    for i in range(tiles):
        q0 = i * QT
        for k0 in range(q0 // KT * KT, tok, KT):
            tile(keys, q0, k0, False, False)
        rows = pl.ds(q0, QT)
        total = jnp.where(lane < 64, pltpu.roll(acc[0, rows, :], 64, 1), pltpu.roll(acc[1, rows, :], 64, 1))
        value = jnp.where(lane < 64, acc[0, rows, :], acc[1, rows, :])
        att[rows, :] = (value / total).astype(BF16)
        for c in range(q0 // chunk, (q0 + QT) // chunk):

            @pl.when(tp != c)
            def _(c=c):
                pltpu.make_async_remote_copy(
                    src_ref=att.at[pl.ds(c * chunk, chunk)], dst_ref=heads.at[tp],
                    send_sem=hsend.at[c], recv_sem=hrecv.at[tp], device_id={"tp": c},
                ).start()

    for c in range(n_tp):

        @pl.when(tp != c)
        def _(c=c):
            pltpu.make_async_remote_copy(
                src_ref=att.at[pl.ds(c * chunk, chunk)], dst_ref=heads.at[c],
                send_sem=hsend.at[c], recv_sem=hrecv.at[c], device_id={"tp": c},
            ).wait_recv()
            out_ref[:, c * 128 : (c + 1) * 128] = heads[c]

        @pl.when(tp == c)
        def _(c=c):
            out_ref[:, c * 128 : (c + 1) * 128] = att[c * chunk : (c + 1) * chunk, :]

    for c in range(n_tp):

        @pl.when(tp != c)
        def _(c=c):
            pltpu.make_async_remote_copy(
                src_ref=att.at[pl.ds(c * chunk, chunk)], dst_ref=heads.at[c],
                send_sem=hsend.at[c], recv_sem=hrecv.at[c], device_id={"tp": c},
            ).wait_send()

    for parts in halo:
        for copy in parts:
            copy.wait_send()


def mixer(query_rows, key_rows, value_rows, forget_cum, doc_ids):
    n_sp, n_tp = lax.axis_size("sp"), lax.axis_size("tp")
    tok, width = query_rows.shape
    marks = jnp.concatenate(
        [forget_cum, doc_ids.astype(F32)[None, :], jnp.zeros((5, tok), F32)], axis=0
    )
    vmem = pl.BlockSpec(memory_space=pltpu.VMEM)
    dma = pltpu.SemaphoreType.DMA
    return pl.pallas_call(
        functools.partial(mixer_kernel, n_sp, n_tp),
        out_shape=jax.ShapeDtypeStruct((tok // n_tp, width * n_tp), BF16),
        in_specs=[vmem] * 4,
        out_specs=vmem,
        scratch_shapes=[
            pltpu.VMEM((REACH, tok, width), BF16),
            pltpu.VMEM((REACH, tok, width), BF16),
            pltpu.VMEM((REACH, 8, tok), F32),
            pltpu.VMEM((2, tok, 2 * width), BF16),
            pltpu.VMEM((tok, width), BF16),
            pltpu.VMEM((2, tok, width), BF16),
            pltpu.VMEM((2, tok, 128), F32),
            pltpu.VMEM((2, tok, 128), F32),
            pltpu.VMEM((tok, width), BF16),
            pltpu.VMEM((n_tp, tok // n_tp, width), BF16),
            dma((REACH,)), dma((REACH,)), dma((REACH,)), dma((REACH,)), dma((REACH,)), dma((REACH,)),
            dma((n_tp,)), dma((n_tp,)),
        ],
        compiler_params=pltpu.CompilerParams(
            collective_id=0, has_side_effects=True, vmem_limit_bytes=48 * 1024 * 1024
        ),
        name="mixer",
    )(query_rows, key_rows, value_rows, marks)


def per_device(
    query_rows,
    key_rows,
    value_rows,
    forget_cum,
    doc_ids,
    residual,
    out_weight,
    norm_gain,
    expert_ids,
    route_weights,
    gate_proj,
    up_proj,
    down_proj,
):
    tok_loc = residual.shape[0]
    token_heads = mixer(query_rows, key_rows, value_rows, forget_cum, doc_ids)
    mixed = jnp.dot(token_heads, out_weight, preferred_element_type=jnp.float32)
    hidden = residual.astype(jnp.float32) + mixed
    normed = (
        hidden * lax.rsqrt(jnp.mean(hidden * hidden, axis=-1, keepdims=True) + norm_eps) * norm_gain
    ).astype(jnp.bfloat16)
    experts = lax.axis_size("sp")
    groups = experts // EPG
    capacity = max(2, 5 * tok_loc // (4 * groups))
    width = normed.shape[1]
    flat = expert_ids.reshape(-1)
    onehot = (flat[:, None] == jnp.arange(experts, dtype=jnp.int32)[None, :]).astype(jnp.int32)
    earlier = jnp.cumsum(onehot, axis=0) - onehot
    slot_rank = jnp.sum(earlier * onehot, axis=1)
    slot = flat * capacity + slot_rank
    select = (jnp.arange(experts * capacity, dtype=jnp.int32)[:, None] == slot[None, :]).astype(
        jnp.bfloat16
    )
    select_tokens = select.reshape(experts * capacity, tok_loc, TOPK).sum(axis=-1)
    sent = jnp.dot(select_tokens, normed, preferred_element_type=jnp.float32).astype(jnp.bfloat16)
    sent = sent.reshape(experts, capacity, width)
    arrived = lax.all_to_all(sent, "sp", split_axis=0, concat_axis=0, tiled=True)
    rows = arrived.reshape(-1, width)
    gate = jnp.dot(rows, gate_proj[0], preferred_element_type=jnp.float32)
    up = jnp.dot(rows, up_proj[0], preferred_element_type=jnp.float32)
    act = (jax.nn.silu(gate) * up).astype(jnp.bfloat16)
    outcome = jnp.dot(act, down_proj[0], preferred_element_type=jnp.float32).astype(jnp.bfloat16)
    back = lax.all_to_all(
        outcome.reshape(arrived.shape), "sp", split_axis=0, concat_axis=0, tiled=True
    )
    back_rows = back.reshape(experts * capacity, width)
    picked = lax.dot_general(
        select, back_rows, (((0,), (0,)), ((), ())), preferred_element_type=jnp.float32
    )
    picked = picked.reshape(tok_loc, TOPK, width)
    combined = jnp.sum(picked * route_weights[:, :, None], axis=1)
    return (hidden + combined).astype(jnp.bfloat16)


def solution(mesh):
    placed = (
        P("sp", "tp"),
        P("sp", "tp"),
        P("sp", "tp"),
        P("tp", "sp"),
        P("sp"),
        P(("sp", "tp"), None),
        P(),
        P(),
        P(("sp", "tp"), None),
        P(("sp", "tp"), None),
        P("sp", None, None),
        P("sp", None, None),
        P("sp", None, None),
    )
    return jax.shard_map(
        per_device, mesh=mesh, in_specs=placed, out_specs=P(("sp", "tp"), None), check_vma=False
    )
```

```python
import functools
import jax
import jax.numpy as jnp
from jax import lax
from jax.experimental import pallas as pl
from jax.experimental.pallas import tpu as pltpu
from jax.sharding import PartitionSpec as P

EPG = 4
TOPK = 2
REACH = 3
QT = 256
KT = 512
FAR = -1e30

norm_eps = 1e-06
F32 = jnp.float32
BF16 = jnp.bfloat16


def columns_of(rows):
    parts = [jnp.transpose(rows[:, c : c + 128]) for c in range(0, rows.shape[1], 128)]
    return jnp.concatenate(parts, axis=0).astype(BF16)


def mixer_kernel(
    n_sp, n_tp, q_ref, k_ref, v_ref, marks_ref, out_ref,
    kbuf, vbuf, mbuf, qaug, kmark, vaug, top, acc, att, heads,
    ksend, krecv, vsend, vrecv, msend, mrecv, hsend, hrecv,
):
    sp = lax.axis_index("sp")
    tp = lax.axis_index("tp")
    tok = q_ref.shape[0]
    chunk = tok // n_tp

    barrier = pltpu.get_barrier_semaphore()
    for d in range(1, REACH + 1):
        for other in (lax.rem(sp + d, n_sp), lax.rem(sp + n_sp - d, n_sp)):
            pl.semaphore_signal(barrier, inc=1, device_id={"sp": other})
    for d in range(1, n_tp):
        pl.semaphore_signal(barrier, inc=1, device_id={"tp": lax.rem(tp + d, n_tp)})
    pl.semaphore_wait(barrier, 2 * REACH + n_tp - 1)

    halo = []
    for d in range(1, REACH + 1):
        ahead = {"sp": lax.rem(sp + d, n_sp)}
        parts = []
        for src, buf, send, recv in (
            (marks_ref, mbuf, msend, mrecv), (k_ref, kbuf, ksend, krecv), (v_ref, vbuf, vsend, vrecv)
        ):
            copy = pltpu.make_async_remote_copy(
                src_ref=src, dst_ref=buf.at[d - 1], send_sem=send.at[d - 1], recv_sem=recv.at[d - 1],
                device_id=ahead,
            )
            copy.start()
            parts.append(copy)
        halo.append(parts)

    lane = lax.broadcasted_iota(jnp.int32, (1, 128), 1)
    row8 = lax.broadcasted_iota(jnp.int32, (8, tok), 0)
    row16 = lax.broadcasted_iota(jnp.int32, (16, tok), 0).astype(F32)
    blank = jnp.zeros((104, tok), F32)
    own = marks_ref[...]
    base = own[0:2, 0:1]

    same = (own[2:3, :] == row16).astype(F32)
    qmark = columns_of(jnp.concatenate([jnp.zeros((8, tok), F32), same, blank], axis=0))
    qrows = q_ref[...] * jnp.asarray(0.125, BF16)
    for h in range(2):
        mine = (lane >= 64 * h) & (lane < 64 * h + 64)
        ones = (lane >= 3 * h) & (lane < 3 * h + 3)
        qaug[h, :, 0:128] = jnp.where(mine, qrows, jnp.zeros_like(qrows))
        qaug[h, :, 128:256] = jnp.where(ones, jnp.ones_like(qmark), qmark)

    def prepare(marks, v):
        gate = base - marks[0:2, :]
        high = gate.astype(BF16).astype(F32)
        rest = gate - high
        mid = rest.astype(BF16).astype(F32)
        low = rest - mid
        pieces = jnp.zeros((8, tok), F32)
        for h in range(2):
            for i, piece in enumerate((high, mid, low)):
                pieces = jnp.where(row8 == 3 * h + i, piece[h : h + 1, :], pieces)
        other = jnp.where(marks[2:3, :] == row16, 0.0, FAR).astype(F32)
        kmark[...] = columns_of(jnp.concatenate([pieces, other, blank], axis=0))
        one = jnp.ones_like(v)
        vaug[0] = jnp.where(lane < 64, v, one)
        vaug[1] = jnp.where(lane < 64, one, v)

    def tile(keys, q0, k0, fresh, causal):
        rows = pl.ds(q0, QT)
        kk = jnp.concatenate([keys[pl.ds(k0, KT), :], kmark[pl.ds(k0, KT), :]], axis=1)
        for h in range(2):
            score = lax.dot_general(
                qaug[h, rows, :], kk, (((1,), (1,)), ((), ())), preferred_element_type=F32
            )
            if causal:
                qpos = q0 + lax.broadcasted_iota(jnp.int32, (QT, KT), 0)
                kpos = k0 + lax.broadcasted_iota(jnp.int32, (QT, KT), 1)
                score = jnp.where(kpos <= qpos, score, FAR)
            best = jnp.broadcast_to(jnp.max(score, axis=1, keepdims=True), (QT, 128))
            if not fresh:
                old = top[h, rows, :]
                best = jnp.maximum(best, old)
            expo = jnp.exp(score - jnp.concatenate([best] * (KT // 128), axis=1)).astype(BF16)
            part = jnp.dot(expo, vaug[h, pl.ds(k0, KT), :], preferred_element_type=F32)
            if not fresh:
                part = acc[h, rows, :] * jnp.exp(old - best) + part
            top[h, rows, :] = best
            acc[h, rows, :] = part

    prepare(own, v_ref[...])
    tiles = tok // QT
    per = KT // QT
    for k0 in range(0, tok, KT):
        first = k0 // QT

        def diagonal(i, carry, k0=k0):
            tile(k_ref, pl.multiple_of(i * QT, QT), k0, k0 == 0, True)
            return carry

        def below(i, carry, k0=k0):
            tile(k_ref, pl.multiple_of(i * QT, QT), k0, k0 == 0, False)
            return carry

        lax.fori_loop(first, first + per, diagonal, 0)
        if first + per < tiles:
            lax.fori_loop(first + per, tiles, below, 0)

    for d in range(1, REACH + 1):
        for copy in halo[d - 1]:
            copy.wait_recv()
        prepare(mbuf[d - 1], vbuf[d - 1])
        keys = kbuf.at[d - 1]
        if d < REACH:

            def full(i, carry, keys=keys):
                for k0 in range(0, tok, KT):
                    tile(keys, pl.multiple_of(i * QT, QT), k0, False, False)
                return carry

            lax.fori_loop(0, tiles, full, 0)

    keys = kbuf.at[REACH - 1]
    sends = []
    for i in range(tiles):
        q0 = i * QT
        for k0 in range(q0 // KT * KT, tok, KT):
            tile(keys, q0, k0, False, False)
        rows = pl.ds(q0, QT)
        total = jnp.where(lane < 64, pltpu.roll(acc[0, rows, :], 64, 1), pltpu.roll(acc[1, rows, :], 64, 1))
        value = jnp.where(lane < 64, acc[0, rows, :], acc[1, rows, :])
        att[rows, :] = (value / total).astype(BF16)
        for c in range(q0 // chunk, (q0 + QT) // chunk):

            @pl.when(tp != c)
            def _(c=c):
                pltpu.make_async_remote_copy(
                    src_ref=att.at[pl.ds(c * chunk, chunk)], dst_ref=heads.at[tp],
                    send_sem=hsend.at[c], recv_sem=hrecv.at[tp], device_id={"tp": c},
                ).start()

    for c in range(n_tp):

        @pl.when(tp != c)
        def _(c=c):
            pltpu.make_async_remote_copy(
                src_ref=att.at[pl.ds(c * chunk, chunk)], dst_ref=heads.at[c],
                send_sem=hsend.at[c], recv_sem=hrecv.at[c], device_id={"tp": c},
            ).wait_recv()
            out_ref[:, c * 128 : (c + 1) * 128] = heads[c]

        @pl.when(tp == c)
        def _(c=c):
            out_ref[:, c * 128 : (c + 1) * 128] = att[c * chunk : (c + 1) * chunk, :]

    for c in range(n_tp):

        @pl.when(tp != c)
        def _(c=c):
            pltpu.make_async_remote_copy(
                src_ref=att.at[pl.ds(c * chunk, chunk)], dst_ref=heads.at[c],
                send_sem=hsend.at[c], recv_sem=hrecv.at[c], device_id={"tp": c},
            ).wait_send()

    for parts in halo:
        for copy in parts:
            copy.wait_send()


def mixer(query_rows, key_rows, value_rows, forget_cum, doc_ids):
    n_sp, n_tp = lax.axis_size("sp"), lax.axis_size("tp")
    tok, width = query_rows.shape
    marks = jnp.concatenate(
        [forget_cum, doc_ids.astype(F32)[None, :], jnp.zeros((5, tok), F32)], axis=0
    )
    vmem = pl.BlockSpec(memory_space=pltpu.VMEM)
    dma = pltpu.SemaphoreType.DMA
    return pl.pallas_call(
        functools.partial(mixer_kernel, n_sp, n_tp),
        out_shape=jax.ShapeDtypeStruct((tok // n_tp, width * n_tp), BF16),
        in_specs=[vmem] * 4,
        out_specs=vmem,
        scratch_shapes=[
            pltpu.VMEM((REACH, tok, width), BF16),
            pltpu.VMEM((REACH, tok, width), BF16),
            pltpu.VMEM((REACH, 8, tok), F32),
            pltpu.VMEM((2, tok, 2 * width), BF16),
            pltpu.VMEM((tok, width), BF16),
            pltpu.VMEM((2, tok, width), BF16),
            pltpu.VMEM((2, tok, 128), F32),
            pltpu.VMEM((2, tok, 128), F32),
            pltpu.VMEM((tok, width), BF16),
            pltpu.VMEM((n_tp, tok // n_tp, width), BF16),
            dma((REACH,)), dma((REACH,)), dma((REACH,)), dma((REACH,)), dma((REACH,)), dma((REACH,)),
            dma((n_tp,)), dma((n_tp,)),
        ],
        compiler_params=pltpu.CompilerParams(
            collective_id=0, has_side_effects=True, vmem_limit_bytes=48 * 1024 * 1024
        ),
        name="mixer",
    )(query_rows, key_rows, value_rows, marks)


HOPS = (0, 1, 7, 2, 6, 3, 5, 4)
PAIRS = len(HOPS) // 2


def stack(blocks):
    parts = []
    for block in blocks:
        parts += [block.astype(F32), jnp.zeros((64 - block.shape[0], block.shape[1]), F32)]
    return jnp.concatenate(parts, axis=0).astype(BF16)


def expert_kernel(
    capacity, heads_ref, residual_ref, gain_ref, route_ref, mix_hbm, gate_hbm, up_hbm, down_hbm, out_ref,
    mix, wgate, wup, wdown, hidden, normed, zs, zbuf, ms, mbuf, mcol, xs, xbuf, ys, ybuf, cs, cbuf,
    load, zsend, zrecv, msend, mrecv, xsend, xrecv, ysend, yrecv, csend, crecv,
):
    sp = lax.axis_index("sp")
    x = lax.rem(sp, EPG)
    z = sp // EPG
    planes = len(HOPS)
    group = 2 * capacity
    tok, width = residual_ref.shape
    ffe = wgate.shape[1]

    def along_z(hop):
        return {"sp": lax.rem(z + hop, planes) * EPG + x}

    def along_x(hop):
        return {"sp": z * EPG + lax.rem(x + hop, EPG)}

    barrier = pltpu.get_barrier_semaphore()
    for hop in range(1, planes):
        pl.semaphore_signal(barrier, inc=1, device_id=along_z(hop))
    for hop in range(1, EPG):
        pl.semaphore_signal(barrier, inc=1, device_id=along_x(hop))

    loads = [
        pltpu.make_async_copy(src, dst, load.at[i])
        for i, (src, dst) in enumerate(
            ((mix_hbm, mix), (gate_hbm, wgate), (up_hbm, wup), (down_hbm, wdown))
        )
    ]
    for copy in loads:
        copy.start()

    ids = route_ref[0:2, :].astype(jnp.int32)
    id0, id1 = ids[0:1, :], ids[1:2, :]
    earlier = (
        lax.broadcasted_iota(jnp.int32, (tok, tok), 0) < lax.broadcasted_iota(jnp.int32, (tok, tok), 1)
    ).astype(BF16)
    number = lax.broadcasted_iota(jnp.int32, (planes * EPG, tok), 0)
    uses = ((number == id0) | (number == id1)).astype(F32)
    rank = jnp.dot(uses.astype(BF16), earlier, preferred_element_type=F32)
    row = lax.broadcasted_iota(jnp.int32, (16, tok), 0)
    which = lax.rem(x + row, EPG)
    pick = (
        (lax.broadcasted_iota(jnp.int32, (16, planes * EPG), 1) & (EPG - 1))
        == lax.rem(x + lax.broadcasted_iota(jnp.int32, (16, planes * EPG), 0), EPG)
    ).astype(BF16)
    slots = jnp.dot(pick, (uses * (rank + 1.0)).astype(BF16), preferred_element_type=F32)
    weight = jnp.where((id0 & (EPG - 1)) == which, route_ref[2:3, :], 0.0) + jnp.where(
        (id1 & (EPG - 1)) == which, route_ref[3:4, :], 0.0
    )
    high = weight.astype(BF16).astype(F32)
    info = jnp.where(row < 4, slots, jnp.where(row < 8, high, jnp.where(row < 12, weight - high, 0.0)))
    info = info.astype(BF16)
    mine = lax.shift_right_logical(id0, 2)
    member = (lax.broadcasted_iota(jnp.int32, (planes, tok), 0) == mine).astype(F32)
    place = jnp.sum(
        member * jnp.dot(member.astype(BF16), earlier, preferred_element_type=F32), axis=0, keepdims=True
    )
    mine = mine.astype(F32)
    spot = lax.broadcasted_iota(jnp.int32, (group, tok), 0).astype(F32)
    sel = []
    for hop in HOPS:
        there = lax.rem(z + hop, planes).astype(F32)
        sel.append(jnp.where((mine == there) & (place == spot), 1.0, 0.0))
    for s in range(planes):
        table = lax.dot_general(
            info, sel[s].astype(BF16), (((1,), (1,)), ((), ())), preferred_element_type=F32
        )
        rest = jnp.zeros((16, 64 - group), F32)
        table = [table, rest, jnp.zeros((16, 64), F32)] if s % 2 == 0 else [jnp.zeros((16, 64), F32), table, rest]
        table = jnp.concatenate(table, axis=1)
        if s == 0:
            mbuf[0] = table
        else:
            ms[s] = table
    sel = jnp.concatenate(sel, axis=0).astype(BF16)
    wide = lax.broadcasted_iota(jnp.int32, (tok, tok), 0)
    cols = jnp.transpose(jnp.where(wide == 0, mine, jnp.where(wide == 1, place, 0.0)))

    loads[0].wait()
    square = jnp.zeros((tok, 128), F32)
    for c in range(0, width, 512):
        part = jnp.dot(heads_ref[...], mix[:, c : c + 512], preferred_element_type=F32)
        part = part + residual_ref[:, c : c + 512].astype(F32)
        hidden[:, c : c + 512] = part
        for i in range(0, 512, 128):
            square = square + part[:, i : i + 128] * part[:, i : i + 128]
    scale = lax.rsqrt(jnp.sum(square, axis=1, keepdims=True) / width + norm_eps)
    for c in range(0, width, 512):
        normed[:, c : c + 512] = (
            hidden[:, c : c + 512] * scale * gain_ref[:, c : c + 512]
        ).astype(BF16)

    for c in range(0, width, 512):
        part = jnp.dot(sel, normed[:, c : c + 512], preferred_element_type=F32)
        zbuf[0, :, c : c + 512] = part[0:group].astype(BF16)
        for s in range(1, planes):
            zs[s, :, c : c + 512] = part[s * group : (s + 1) * group].astype(BF16)
    pl.semaphore_wait(barrier, planes + EPG - 2)

    def zcopy(s):
        return pltpu.make_async_remote_copy(
            src_ref=zs.at[s], dst_ref=zbuf.at[s], send_sem=zsend.at[s], recv_sem=zrecv.at[s],
            device_id=along_z(HOPS[s]),
        )

    def mcopy(s):
        return pltpu.make_async_remote_copy(
            src_ref=ms.at[s], dst_ref=mbuf.at[s], send_sem=msend.at[s], recv_sem=mrecv.at[s],
            device_id=along_z(HOPS[s]),
        )

    def xcopy(p, hop):
        return pltpu.make_async_remote_copy(
            src_ref=xs.at[p, hop], dst_ref=xbuf.at[p, hop], send_sem=xsend.at[p, hop],
            recv_sem=xrecv.at[p, hop], device_id=along_x(hop),
        )

    def ycopy(p, hop):
        return pltpu.make_async_remote_copy(
            src_ref=ys.at[p, hop], dst_ref=ybuf.at[p, hop], send_sem=ysend.at[p, hop],
            recv_sem=yrecv.at[p, hop], device_id=along_x(EPG - hop),
        )

    def ccopy(s):
        return pltpu.make_async_remote_copy(
            src_ref=cs.at[s], dst_ref=cbuf.at[s], send_sem=csend.at[s], recv_sem=crecv.at[s],
            device_id=along_z(planes - HOPS[s]),
        )

    for s in range(1, planes):
        mcopy(s).start()
        zcopy(s).start()

    def spread(p):
        for half in range(2):
            s = 2 * p + half
            if s:
                mcopy(s).wait_recv()
            table = jnp.concatenate([mbuf[s], jnp.zeros((112, 128), F32)], axis=0)
            mcol[s] = jnp.transpose(table)[64 * half : 64 * half + group, :]
        second = mbuf[2 * p + 1]
        table = mbuf[2 * p] + jnp.where(second > 0.0, second + float(capacity), 0.0)
        want = lax.broadcasted_iota(jnp.int32, (group, 128), 0).astype(F32) + 1.0
        rows = [jnp.where(table[h : h + 1, :] == want, 1.0, 0.0) for h in range(EPG)]
        order = jnp.concatenate(rows, axis=0).astype(BF16)
        for half in range(2):
            if 2 * p + half:
                zcopy(2 * p + half).wait_recv()
        for c in range(0, width, 512):
            rows = stack([zbuf[2 * p, :, c : c + 512], zbuf[2 * p + 1, :, c : c + 512]])
            part = jnp.dot(order, rows, preferred_element_type=F32)
            xbuf[p, 0, :, c : c + 512] = part[0:group].astype(BF16)
            for h in range(1, EPG):
                xs[p, h, :, c : c + 512] = part[h * group : (h + 1) * group].astype(BF16)
        for h in range(1, EPG):
            xcopy(p, h).start()

    def expert(p):
        for h in range(1, EPG):
            xcopy(p, h).wait_recv()
        gate = jnp.zeros((EPG * group, ffe), F32)
        up = jnp.zeros((EPG * group, ffe), F32)
        for c in range(0, width, 512):
            rows = jnp.concatenate(
                [xbuf[p, h, :, c : c + 512].astype(F32) for h in range(EPG)], axis=0
            ).astype(BF16)
            gate = gate + jnp.dot(rows, wgate[c : c + 512, :], preferred_element_type=F32)
            up = up + jnp.dot(rows, wup[c : c + 512, :], preferred_element_type=F32)
        act = (gate / (1.0 + jnp.exp(-gate)) * up).astype(BF16)
        for c in range(0, width, 512):
            part = jnp.dot(act, wdown[:, c : c + 512], preferred_element_type=F32)
            ybuf[p, 0, :, c : c + 512] = part[0:group].astype(BF16)
            for h in range(1, EPG):
                ys[p, h, :, c : c + 512] = part[h * group : (h + 1) * group].astype(BF16)
        for h in range(1, EPG):
            ycopy(p, h).start()

    def collect(p):
        lanes = lax.broadcasted_iota(jnp.int32, (group, 128), 1)
        left = lanes < 64
        want = ((lanes & 63) + 1).astype(F32)
        mats = []
        for h in range(0, EPG, 2):
            parts = []
            for kind in (4, 8):
                for half in range(2):
                    col = mcol[2 * p + half]
                    goal = jnp.where(left, col[:, h : h + 1], col[:, h + 1 : h + 2])
                    goal = jnp.where(goal > 0.0, goal + float(half * capacity), 0.0)
                    share = jnp.where(left, col[:, kind + h : kind + h + 1], col[:, kind + h + 1 : kind + h + 2])
                    parts.append(jnp.where(goal == want, share, 0.0))
            mats.append(jnp.concatenate(parts, axis=0))
        mats = jnp.concatenate(mats, axis=1).astype(BF16)
        for h in range(1, EPG):
            ycopy(p, h).wait_recv()
        for c in range(0, width, 512):
            rows = stack([ybuf[p, h, :, c : c + 512] for h in range(EPG)])
            part = jnp.dot(mats, rows, preferred_element_type=F32)
            for half in range(2):
                both = part[half * group : (half + 1) * group] + part[(2 + half) * group : (3 + half) * group]
                s = 2 * p + half
                if s:
                    cs[s, :, c : c + 512] = both.astype(BF16)
                else:
                    cbuf[0, :, c : c + 512] = both.astype(BF16)
        for half in range(2):
            if 2 * p + half:
                ccopy(2 * p + half).start()

    spread(0)
    spread(1)
    for copy in loads[1:]:
        copy.wait()
    expert(0)
    spread(2)
    expert(1)
    collect(0)
    spread(3)
    expert(2)
    collect(1)
    expert(3)
    collect(2)
    collect(3)
    lanes = lax.broadcasted_iota(jnp.int32, (tok, 128), 1)
    back = []
    for p in range(PAIRS):
        there = jnp.where(lanes < 64, lax.rem(z + HOPS[2 * p], planes), lax.rem(z + HOPS[2 * p + 1], planes))
        hit = (cols[:, 0:1] == there.astype(F32)) & (cols[:, 1:2] == (lanes & 63).astype(F32))
        back.append(jnp.where(hit, 1.0, 0.0))
    back = jnp.concatenate(back, axis=1).astype(BF16)
    for s in range(1, planes):
        ccopy(s).wait_recv()
    for c in range(0, width, 512):
        rows = stack([cbuf[s, :, c : c + 512] for s in range(planes)])
        part = jnp.dot(back, rows, preferred_element_type=F32)
        out_ref[:, c : c + 512] = (hidden[:, c : c + 512] + part).astype(BF16)

    for s in range(1, planes):
        mcopy(s).wait_send()
        zcopy(s).wait_send()
        ccopy(s).wait_send()
    for p in range(PAIRS):
        for h in range(1, EPG):
            xcopy(p, h).wait_send()
            ycopy(p, h).wait_send()


def experts_layer(heads, residual, out_weight, norm_gain, expert_ids, route_weights, gate, up, down):
    tok, width = residual.shape
    ffe = gate.shape[1]
    planes = lax.axis_size("sp") // EPG
    capacity = max(2, 5 * tok // (4 * planes))
    group = 2 * capacity
    route = jnp.concatenate(
        [expert_ids.T.astype(F32), route_weights.T, jnp.zeros((4, tok), F32)], axis=0
    )
    vmem = pl.BlockSpec(memory_space=pltpu.VMEM)
    hbm = pl.BlockSpec(memory_space=pl.ANY)
    dma = pltpu.SemaphoreType.DMA
    slots = pltpu.VMEM((planes, group, width), BF16)
    quads = pltpu.VMEM((PAIRS, EPG, group, width), BF16)
    return pl.pallas_call(
        functools.partial(expert_kernel, capacity),
        out_shape=jax.ShapeDtypeStruct((tok, width), BF16),
        in_specs=[vmem] * 4 + [hbm] * 4,
        out_specs=vmem,
        scratch_shapes=[
            pltpu.VMEM(out_weight.shape, BF16),
            pltpu.VMEM(gate.shape, BF16),
            pltpu.VMEM(up.shape, BF16),
            pltpu.VMEM(down.shape, BF16),
            pltpu.VMEM((tok, width), F32),
            pltpu.VMEM((tok, width), BF16),
            slots, slots,
            pltpu.VMEM((planes, 16, 128), F32),
            pltpu.VMEM((planes, 16, 128), F32),
            pltpu.VMEM((planes, group, 128), F32),
            quads, quads, quads, quads,
            slots, slots,
            dma((4,)),
            dma((planes,)), dma((planes,)), dma((planes,)), dma((planes,)),
            dma((PAIRS, EPG)), dma((PAIRS, EPG)), dma((PAIRS, EPG)), dma((PAIRS, EPG)),
            dma((planes,)), dma((planes,)),
        ],
        compiler_params=pltpu.CompilerParams(
            collective_id=1, has_side_effects=True, vmem_limit_bytes=60 * 1024 * 1024
        ),
        name="experts",
    )(heads, residual, norm_gain[None, :], route, out_weight, gate, up, down)


def per_device(
    query_rows,
    key_rows,
    value_rows,
    forget_cum,
    doc_ids,
    residual,
    out_weight,
    norm_gain,
    expert_ids,
    route_weights,
    gate_proj,
    up_proj,
    down_proj,
):
    heads = mixer(query_rows, key_rows, value_rows, forget_cum, doc_ids)
    return experts_layer(
        heads, residual, out_weight, norm_gain, expert_ids, route_weights, gate_proj[0], up_proj[0], down_proj[0]
    )


def solution(mesh):
    placed = (
        P("sp", "tp"),
        P("sp", "tp"),
        P("sp", "tp"),
        P("tp", "sp"),
        P("sp"),
        P(("sp", "tp"), None),
        P(),
        P(),
        P(("sp", "tp"), None),
        P(("sp", "tp"), None),
        P("sp", None, None),
        P("sp", None, None),
        P("sp", None, None),
    )
    return jax.shard_map(
        per_device, mesh=mesh, in_specs=placed, out_specs=P(("sp", "tp"), None), check_vma=False
    )
```

```python
import functools
import jax
import jax.numpy as jnp
from jax import lax
from jax.experimental import pallas as pl
from jax.experimental.pallas import tpu as pltpu
from jax.sharding import PartitionSpec as P

EPG = 4
TOPK = 2
REACH = 3
QT = 512
QF = 1024
KT = 512
FAR = -1e30
CUTS = 2
STRAIGHT = ()

norm_eps = 1e-06
F32 = jnp.float32
BF16 = jnp.bfloat16


def columns_of(rows):
    parts = [jnp.transpose(rows[:, c : c + 128]) for c in range(0, rows.shape[1], 128)]
    return jnp.concatenate(parts, axis=0).astype(BF16)


def mixer_kernel(
    n_sp, n_tp, q_hbm, k_hbm, v_hbm, gate_ref, doc_ref, out_ref,
    q_ref, k_ref, v_ref, marks_ref, krel, vrel, mrel,
    kbuf, vbuf, mbuf, qaug, keyt, vaug, top, acc, att, heads,
    load, rsend, rrecv, hsend, hrecv, asend, arecv,
):
    sp = lax.axis_index("sp")
    tp = lax.axis_index("tp")
    tok = q_ref.shape[0]
    chunk = tok // n_tp

    x = lax.rem(sp, EPG)
    z = sp // EPG
    planes = n_sp // EPG

    def along_x(hop):
        return {"sp": z * EPG + lax.rem(x + hop, EPG)}

    def along_z(hop):
        return {"sp": lax.rem(z + hop, planes) * EPG + x}

    barrier = pltpu.get_barrier_semaphore()
    for hop in range(1, EPG):
        pl.semaphore_signal(barrier, inc=1, device_id=along_x(hop))
    for hop in (1, planes - 1):
        pl.semaphore_signal(barrier, inc=1, device_id=along_z(hop))
    for d in range(1, REACH + 1):
        for other in (lax.rem(sp + d, n_sp), lax.rem(sp + n_sp - d, n_sp)):
            pl.semaphore_signal(barrier, inc=1, device_id={"sp": other})
    for d in range(1, n_tp):
        pl.semaphore_signal(barrier, inc=1, device_id={"tp": lax.rem(tp + d, n_tp)})

    loads = [
        pltpu.make_async_copy(src, dst, load.at[i])
        for i, (src, dst) in enumerate(((k_hbm, k_ref), (v_hbm, v_ref), (q_hbm, q_ref)))
    ]
    for copy in loads:
        copy.start()
    marks_ref[...] = jnp.concatenate(
        [gate_ref[...], doc_ref[...].astype(F32), jnp.zeros((5, tok), F32)], axis=0
    )
    pl.semaphore_wait(barrier, EPG - 1 + 2 + 2 * REACH + n_tp - 1)

    part = tok // CUTS
    pieces = [(marks_ref, mrel, mbuf, None)]
    for src, rel, buf in ((k_ref, krel, kbuf), (v_ref, vrel, vbuf)):
        pieces += [(src, rel, buf, pl.ds(c * part, part)) for c in range(CUTS)]

    def across(i):
        src, rel, buf, rows = pieces[i]
        if rows is not None:
            src, rel = src.at[rows], rel.at[rows]
        return pltpu.make_async_remote_copy(
            src_ref=src, dst_ref=rel, send_sem=rsend.at[i], recv_sem=rrecv.at[i], device_id=along_z(1)
        )

    def along(i, d, relayed):
        src, rel, buf, rows = pieces[i]
        src = rel if relayed else src
        dst = buf.at[d - 1]
        if rows is not None:
            src, dst = src.at[rows], dst.at[rows]
        return pltpu.make_async_remote_copy(
            src_ref=src, dst_ref=dst, send_sem=hsend.at[d - 1, i], recv_sem=hrecv.at[d - 1, i],
            device_id=along_x(d) if relayed else {"sp": lax.rem(sp + d, n_sp)},
        )

    def straight(d):
        here = x + d < EPG
        for column, far in STRAIGHT:
            if far == d:
                here = here | (x == column)
        return here

    relays = sorted({c for c in range(1, EPG) for d in range(EPG - c, EPG) if (c, d) not in STRAIGHT})

    def relaying():
        here = x == relays[0]
        for c in relays[1:]:
            here = here | (x == c)
        return here

    for i in range(len(pieces)):
        if i in (1, 1 + CUTS):
            loads[0 if i == 1 else 1].wait()

        @pl.when(relaying())
        def _(i=i):
            across(i).start()

        for d in range(1, REACH + 1):

            @pl.when(straight(d))
            def _(i=i, d=d):
                along(i, d, False).start()

    loads[2].wait()

    def pass_on(i):
        @pl.when(relaying())
        def _():
            across(i).wait_recv()

        for d in range(1, REACH + 1):

            @pl.when(jnp.logical_not(straight(d)))
            def _(d=d):
                along(i, d, True).start()

    lane = lax.broadcasted_iota(jnp.int32, (1, 128), 1)
    row8 = lax.broadcasted_iota(jnp.int32, (8, tok), 0)
    row16 = lax.broadcasted_iota(jnp.int32, (16, tok), 0).astype(F32)
    blank = jnp.zeros((104, tok), F32)
    own = marks_ref[...]
    base = own[0:2, 0:1]

    same = (own[2:3, :] == row16).astype(F32)
    qmark = columns_of(jnp.concatenate([jnp.zeros((8, tok), F32), same, blank], axis=0))
    qrows = q_ref[...] * jnp.asarray(0.125, BF16)
    for h in range(2):
        mine = (lane >= 64 * h) & (lane < 64 * h + 64)
        ones = (lane >= 3 * h) & (lane < 3 * h + 3)
        qaug[h, :, 0:128] = jnp.where(mine, qrows, jnp.zeros_like(qrows))
        qaug[h, :, 128:256] = jnp.where(ones, jnp.ones_like(qmark), qmark)

    def prepare(marks, keys, v):
        gate = base - marks[0:2, :]
        high = gate.astype(BF16).astype(F32)
        rest = gate - high
        mid = rest.astype(BF16).astype(F32)
        low = rest - mid
        pieces = jnp.zeros((8, tok), F32)
        for h in range(2):
            for i, piece in enumerate((high, mid, low)):
                pieces = jnp.where(row8 == 3 * h + i, piece[h : h + 1, :], pieces)
        other = jnp.where(marks[2:3, :] == row16, 0.0, FAR).astype(F32)
        keyt[128:256, :] = jnp.concatenate([pieces, other, blank], axis=0).astype(BF16)
        for c in range(0, tok, 128):
            keyt[0:128, c : c + 128] = jnp.transpose(keys[c : c + 128, :].astype(F32)).astype(BF16)
        one = jnp.ones_like(v)
        vaug[0] = jnp.where(lane < 64, v, one)
        vaug[1] = jnp.where(lane < 64, one, v)

    def tile(q0, k0, fresh, causal, wide=QT):
        rows = pl.ds(q0, wide)
        for h in range(2):
            score = jnp.dot(qaug[h, rows, :], keyt[:, pl.ds(k0, KT)], preferred_element_type=F32)
            if causal:
                qpos = q0 + lax.broadcasted_iota(jnp.int32, (wide, KT), 0)
                kpos = k0 + lax.broadcasted_iota(jnp.int32, (wide, KT), 1)
                score = jnp.where(kpos <= qpos, score, FAR)
            best = jnp.broadcast_to(jnp.max(score, axis=1, keepdims=True), (wide, 128))
            if not fresh:
                old = top[h, rows, :]
                best = jnp.maximum(best, old)
            expo = jnp.exp(score - jnp.concatenate([best] * (KT // 128), axis=1)).astype(BF16)
            part = jnp.dot(expo, vaug[h, pl.ds(k0, KT), :], preferred_element_type=F32)
            if not fresh:
                part = acc[h, rows, :] * jnp.exp(old - best) + part
            top[h, rows, :] = best
            acc[h, rows, :] = part

    prepare(own, k_ref, v_ref[...])
    tiles = tok // QT
    per = KT // QT
    for k0 in range(0, tok, KT):
        first = k0 // QT

        def diagonal(i, carry, k0=k0):
            tile(pl.multiple_of(i * QT, QT), k0, k0 == 0, True)
            return carry

        def below(i, carry, k0=k0):
            tile(pl.multiple_of(i * QT, QT), k0, k0 == 0, False)
            return carry

        lax.fori_loop(first, first + per, diagonal, 0)
        if first + per < tiles:
            lax.fori_loop(first + per, tiles, below, 0)

    for i in range(len(pieces)):
        pass_on(i)
    for d in range(1, REACH + 1):
        for i in range(len(pieces)):
            along(i, d, False).wait_recv()
        prepare(mbuf[d - 1], kbuf.at[d - 1], vbuf[d - 1])
        if d < REACH:

            def full(i, carry):
                for k0 in range(0, tok, KT):
                    tile(pl.multiple_of(i * QF, QF), k0, False, False, QF)
                return carry

            lax.fori_loop(0, tok // QF, full, 0)

    for i in range(tiles):
        q0 = i * QT
        for k0 in range(q0 // KT * KT, tok, KT):
            tile(q0, k0, False, False)
        rows = pl.ds(q0, QT)
        total = jnp.where(lane < 64, pltpu.roll(acc[0, rows, :], 64, 1), pltpu.roll(acc[1, rows, :], 64, 1))
        value = jnp.where(lane < 64, acc[0, rows, :], acc[1, rows, :])
        att[rows, :] = (value / total).astype(BF16)
        for c in range(q0 // chunk, (q0 + QT) // chunk):

            @pl.when(tp != c)
            def _(c=c):
                pltpu.make_async_remote_copy(
                    src_ref=att.at[pl.ds(c * chunk, chunk)], dst_ref=heads.at[tp],
                    send_sem=asend.at[c], recv_sem=arecv.at[tp], device_id={"tp": c},
                ).start()

    for c in range(n_tp):

        @pl.when(tp != c)
        def _(c=c):
            pltpu.make_async_remote_copy(
                src_ref=att.at[pl.ds(c * chunk, chunk)], dst_ref=heads.at[c],
                send_sem=asend.at[c], recv_sem=arecv.at[c], device_id={"tp": c},
            ).wait_recv()
            out_ref[:, c * 128 : (c + 1) * 128] = heads[c]

        @pl.when(tp == c)
        def _(c=c):
            out_ref[:, c * 128 : (c + 1) * 128] = att[c * chunk : (c + 1) * chunk, :]

    for c in range(n_tp):

        @pl.when(tp != c)
        def _(c=c):
            pltpu.make_async_remote_copy(
                src_ref=att.at[pl.ds(c * chunk, chunk)], dst_ref=heads.at[c],
                send_sem=asend.at[c], recv_sem=arecv.at[c], device_id={"tp": c},
            ).wait_send()

    for i in range(len(pieces)):

        @pl.when(relaying())
        def _(i=i):
            across(i).wait_send()

        for d in range(1, REACH + 1):
            along(i, d, False).wait_send()


def mixer(query_rows, key_rows, value_rows, forget_cum, doc_ids):
    n_sp, n_tp = lax.axis_size("sp"), lax.axis_size("tp")
    tok, width = query_rows.shape
    vmem = pl.BlockSpec(memory_space=pltpu.VMEM)
    hbm = pl.BlockSpec(memory_space=pl.ANY)
    dma = pltpu.SemaphoreType.DMA
    return pl.pallas_call(
        functools.partial(mixer_kernel, n_sp, n_tp),
        out_shape=jax.ShapeDtypeStruct((tok // n_tp, width * n_tp), BF16),
        in_specs=[hbm] * 3 + [vmem] * 2,
        out_specs=vmem,
        scratch_shapes=[
            pltpu.VMEM((tok, width), BF16),
            pltpu.VMEM((tok, width), BF16),
            pltpu.VMEM((tok, width), BF16),
            pltpu.VMEM((8, tok), F32),
            pltpu.VMEM((tok, width), BF16),
            pltpu.VMEM((tok, width), BF16),
            pltpu.VMEM((8, tok), F32),
            pltpu.VMEM((REACH, tok, width), BF16),
            pltpu.VMEM((REACH, tok, width), BF16),
            pltpu.VMEM((REACH, 8, tok), F32),
            pltpu.VMEM((2, tok, 2 * width), BF16),
            pltpu.VMEM((2 * width, tok), BF16),
            pltpu.VMEM((2, tok, width), BF16),
            pltpu.VMEM((2, tok, 128), F32),
            pltpu.VMEM((2, tok, 128), F32),
            pltpu.VMEM((tok, width), BF16),
            pltpu.VMEM((n_tp, tok // n_tp, width), BF16),
            dma((3,)),
            dma((1 + 2 * CUTS,)), dma((1 + 2 * CUTS,)),
            dma((REACH, 1 + 2 * CUTS)), dma((REACH, 1 + 2 * CUTS)),
            dma((n_tp,)), dma((n_tp,)),
        ],
        compiler_params=pltpu.CompilerParams(
            collective_id=0, has_side_effects=True, vmem_limit_bytes=67043328
        ),
        name="mixer",
    )(query_rows, key_rows, value_rows, forget_cum, doc_ids[None, :])


HOPS = (0, 1, 7, 2, 6, 3, 5, 4)
PAIRS = len(HOPS) // 2


def stack(blocks):
    parts = []
    for block in blocks:
        parts += [block.astype(F32), jnp.zeros((64 - block.shape[0], block.shape[1]), F32)]
    return jnp.concatenate(parts, axis=0).astype(BF16)


def expert_kernel(
    capacity, heads_ref, gain_ref, ids_ref, weights_ref, residual_hbm, mix_hbm, gate_hbm, up_hbm, down_hbm, out_ref,
    residual_ref, mix, wgate, wup, wdown, hidden, normed, zs, zbuf, ms, mbuf, mcol, xs, xbuf, ys, ybuf, cs, cbuf,
    load, zsend, zrecv, msend, mrecv, xsend, xrecv, ysend, yrecv, csend, crecv,
):
    sp = lax.axis_index("sp")
    x = lax.rem(sp, EPG)
    z = sp // EPG
    planes = len(HOPS)
    group = 2 * capacity
    tok, width = residual_ref.shape
    ffe = wgate.shape[1]

    def along_z(hop):
        return {"sp": lax.rem(z + hop, planes) * EPG + x}

    def along_x(hop):
        return {"sp": z * EPG + lax.rem(x + hop, EPG)}

    barrier = pltpu.get_barrier_semaphore()
    for hop in range(1, planes):
        pl.semaphore_signal(barrier, inc=1, device_id=along_z(hop))
    for hop in range(1, EPG):
        pl.semaphore_signal(barrier, inc=1, device_id=along_x(hop))

    loads = [
        pltpu.make_async_copy(src, dst, load.at[i])
        for i, (src, dst) in enumerate(
            ((residual_hbm, residual_ref), (mix_hbm, mix), (gate_hbm, wgate), (up_hbm, wup), (down_hbm, wdown))
        )
    ]
    for copy in loads:
        copy.start()

    ids = ids_ref[...]
    id0, id1 = ids[0:1, :], ids[1:2, :]
    earlier = (
        lax.broadcasted_iota(jnp.int32, (tok, tok), 0) < lax.broadcasted_iota(jnp.int32, (tok, tok), 1)
    ).astype(BF16)
    number = lax.broadcasted_iota(jnp.int32, (planes * EPG, tok), 0)
    uses = ((number == id0) | (number == id1)).astype(F32)
    rank = jnp.dot(uses.astype(BF16), earlier, preferred_element_type=F32)
    row = lax.broadcasted_iota(jnp.int32, (16, tok), 0)
    which = lax.rem(x + row, EPG)
    pick = (
        (lax.broadcasted_iota(jnp.int32, (16, planes * EPG), 1) & (EPG - 1))
        == lax.rem(x + lax.broadcasted_iota(jnp.int32, (16, planes * EPG), 0), EPG)
    ).astype(BF16)
    slots = jnp.dot(pick, (uses * (rank + 1.0)).astype(BF16), preferred_element_type=F32)
    weight = jnp.where((id0 & (EPG - 1)) == which, weights_ref[0:1, :], 0.0) + jnp.where(
        (id1 & (EPG - 1)) == which, weights_ref[1:2, :], 0.0
    )
    high = weight.astype(BF16).astype(F32)
    info = jnp.where(row < 4, slots, jnp.where(row < 8, high, jnp.where(row < 12, weight - high, 0.0)))
    info = info.astype(BF16)
    mine = lax.shift_right_logical(id0, 2)
    member = (lax.broadcasted_iota(jnp.int32, (planes, tok), 0) == mine).astype(F32)
    place = jnp.sum(
        member * jnp.dot(member.astype(BF16), earlier, preferred_element_type=F32), axis=0, keepdims=True
    )
    mine = mine.astype(F32)
    spot = lax.broadcasted_iota(jnp.int32, (group, tok), 0).astype(F32)
    sel = []
    for hop in HOPS:
        there = lax.rem(z + hop, planes).astype(F32)
        sel.append(jnp.where((mine == there) & (place == spot), 1.0, 0.0))
    for s in range(planes):
        table = lax.dot_general(
            info, sel[s].astype(BF16), (((1,), (1,)), ((), ())), preferred_element_type=F32
        )
        rest = jnp.zeros((16, 64 - group), F32)
        table = [table, rest, jnp.zeros((16, 64), F32)] if s % 2 == 0 else [jnp.zeros((16, 64), F32), table, rest]
        table = jnp.concatenate(table, axis=1)
        if s == 0:
            mbuf[0] = table
        else:
            ms[s] = table
    sel = jnp.concatenate(sel, axis=0).astype(BF16)
    wide = lax.broadcasted_iota(jnp.int32, (tok, tok), 0)
    cols = jnp.transpose(jnp.where(wide == 0, mine, jnp.where(wide == 1, place, 0.0)))

    loads[0].wait()
    loads[1].wait()
    square = jnp.zeros((tok, 128), F32)
    for c in range(0, width, 512):
        part = jnp.dot(heads_ref[...], mix[:, c : c + 512], preferred_element_type=F32)
        part = part + residual_ref[:, c : c + 512].astype(F32)
        hidden[:, c : c + 512] = part
        for i in range(0, 512, 128):
            square = square + part[:, i : i + 128] * part[:, i : i + 128]
    scale = lax.rsqrt(jnp.sum(square, axis=1, keepdims=True) / width + norm_eps)
    for c in range(0, width, 512):
        normed[:, c : c + 512] = (
            hidden[:, c : c + 512] * scale * gain_ref[:, c : c + 512]
        ).astype(BF16)

    for c in range(0, width, 512):
        part = jnp.dot(sel, normed[:, c : c + 512], preferred_element_type=F32)
        zbuf[0, :, c : c + 512] = part[0:group].astype(BF16)
        for s in range(1, planes):
            zs[s, :, c : c + 512] = part[s * group : (s + 1) * group].astype(BF16)
    pl.semaphore_wait(barrier, planes + EPG - 2)

    def zcopy(s):
        return pltpu.make_async_remote_copy(
            src_ref=zs.at[s], dst_ref=zbuf.at[s], send_sem=zsend.at[s], recv_sem=zrecv.at[s],
            device_id=along_z(HOPS[s]),
        )

    def mcopy(s):
        return pltpu.make_async_remote_copy(
            src_ref=ms.at[s], dst_ref=mbuf.at[s], send_sem=msend.at[s], recv_sem=mrecv.at[s],
            device_id=along_z(HOPS[s]),
        )

    def xcopy(p, hop):
        return pltpu.make_async_remote_copy(
            src_ref=xs.at[p, hop], dst_ref=xbuf.at[p, hop], send_sem=xsend.at[p, hop],
            recv_sem=xrecv.at[p, hop], device_id=along_x(hop),
        )

    def ycopy(p, hop):
        return pltpu.make_async_remote_copy(
            src_ref=ys.at[p, hop], dst_ref=ybuf.at[p, hop], send_sem=ysend.at[p, hop],
            recv_sem=yrecv.at[p, hop], device_id=along_x(EPG - hop),
        )

    def ccopy(s):
        return pltpu.make_async_remote_copy(
            src_ref=cs.at[s], dst_ref=cbuf.at[s], send_sem=csend.at[s], recv_sem=crecv.at[s],
            device_id=along_z(planes - HOPS[s]),
        )

    for s in range(1, planes):
        mcopy(s).start()
        zcopy(s).start()

    def spread(p):
        for half in range(2):
            s = 2 * p + half
            if s:
                mcopy(s).wait_recv()
            table = jnp.concatenate([mbuf[s], jnp.zeros((112, 128), F32)], axis=0)
            mcol[s] = jnp.transpose(table)[64 * half : 64 * half + group, :]
        second = mbuf[2 * p + 1]
        table = mbuf[2 * p] + jnp.where(second > 0.0, second + float(capacity), 0.0)
        want = lax.broadcasted_iota(jnp.int32, (group, 128), 0).astype(F32) + 1.0
        rows = [jnp.where(table[h : h + 1, :] == want, 1.0, 0.0) for h in range(EPG)]
        order = jnp.concatenate(rows, axis=0).astype(BF16)
        for half in range(2):
            if 2 * p + half:
                zcopy(2 * p + half).wait_recv()
        for c in range(0, width, 512):
            rows = stack([zbuf[2 * p, :, c : c + 512], zbuf[2 * p + 1, :, c : c + 512]])
            part = jnp.dot(order, rows, preferred_element_type=F32)
            xbuf[p, 0, :, c : c + 512] = part[0:group].astype(BF16)
            for h in range(1, EPG):
                xs[p, h, :, c : c + 512] = part[h * group : (h + 1) * group].astype(BF16)
        for h in range(1, EPG):
            xcopy(p, h).start()

    def expert(p):
        for h in range(1, EPG):
            xcopy(p, h).wait_recv()
        gate = jnp.zeros((EPG * group, ffe), F32)
        up = jnp.zeros((EPG * group, ffe), F32)
        for c in range(0, width, 512):
            rows = jnp.concatenate(
                [xbuf[p, h, :, c : c + 512].astype(F32) for h in range(EPG)], axis=0
            ).astype(BF16)
            gate = gate + jnp.dot(rows, wgate[c : c + 512, :], preferred_element_type=F32)
            up = up + jnp.dot(rows, wup[c : c + 512, :], preferred_element_type=F32)
        act = (gate / (1.0 + jnp.exp(-gate)) * up).astype(BF16)
        for c in range(0, width, 512):
            part = jnp.dot(act, wdown[:, c : c + 512], preferred_element_type=F32)
            ybuf[p, 0, :, c : c + 512] = part[0:group].astype(BF16)
            for h in range(1, EPG):
                ys[p, h, :, c : c + 512] = part[h * group : (h + 1) * group].astype(BF16)
        for h in range(1, EPG):
            ycopy(p, h).start()

    def collect(p):
        lanes = lax.broadcasted_iota(jnp.int32, (group, 128), 1)
        left = lanes < 64
        want = ((lanes & 63) + 1).astype(F32)
        mats = []
        for h in range(0, EPG, 2):
            parts = []
            for kind in (4, 8):
                for half in range(2):
                    col = mcol[2 * p + half]
                    goal = jnp.where(left, col[:, h : h + 1], col[:, h + 1 : h + 2])
                    goal = jnp.where(goal > 0.0, goal + float(half * capacity), 0.0)
                    share = jnp.where(left, col[:, kind + h : kind + h + 1], col[:, kind + h + 1 : kind + h + 2])
                    parts.append(jnp.where(goal == want, share, 0.0))
            mats.append(jnp.concatenate(parts, axis=0))
        mats = jnp.concatenate(mats, axis=1).astype(BF16)
        for h in range(1, EPG):
            ycopy(p, h).wait_recv()
        for c in range(0, width, 512):
            rows = stack([ybuf[p, h, :, c : c + 512] for h in range(EPG)])
            part = jnp.dot(mats, rows, preferred_element_type=F32)
            for half in range(2):
                both = part[half * group : (half + 1) * group] + part[(2 + half) * group : (3 + half) * group]
                s = 2 * p + half
                if s:
                    cs[s, :, c : c + 512] = both.astype(BF16)
                else:
                    cbuf[0, :, c : c + 512] = both.astype(BF16)
        for half in range(2):
            if 2 * p + half:
                ccopy(2 * p + half).start()

    spread(0)
    spread(1)
    for copy in loads[2:]:
        copy.wait()
    expert(0)
    spread(2)
    expert(1)
    collect(0)
    spread(3)
    expert(2)
    collect(1)
    expert(3)
    collect(2)
    collect(3)
    lanes = lax.broadcasted_iota(jnp.int32, (tok, 128), 1)
    back = []
    for p in range(PAIRS):
        there = jnp.where(lanes < 64, lax.rem(z + HOPS[2 * p], planes), lax.rem(z + HOPS[2 * p + 1], planes))
        hit = (cols[:, 0:1] == there.astype(F32)) & (cols[:, 1:2] == (lanes & 63).astype(F32))
        back.append(jnp.where(hit, 1.0, 0.0))
    back = jnp.concatenate(back, axis=1).astype(BF16)
    for s in range(1, planes):
        ccopy(s).wait_recv()
    for c in range(0, width, 512):
        rows = stack([cbuf[s, :, c : c + 512] for s in range(planes)])
        part = jnp.dot(back, rows, preferred_element_type=F32)
        out_ref[:, c : c + 512] = (hidden[:, c : c + 512] + part).astype(BF16)

    for s in range(1, planes):
        mcopy(s).wait_send()
        zcopy(s).wait_send()
        ccopy(s).wait_send()
    for p in range(PAIRS):
        for h in range(1, EPG):
            xcopy(p, h).wait_send()
            ycopy(p, h).wait_send()


def experts_layer(heads, residual, out_weight, norm_gain, expert_ids, route_weights, gate, up, down):
    tok, width = residual.shape
    ffe = gate.shape[1]
    planes = lax.axis_size("sp") // EPG
    capacity = max(2, 5 * tok // (4 * planes))
    group = 2 * capacity
    vmem = pl.BlockSpec(memory_space=pltpu.VMEM)
    hbm = pl.BlockSpec(memory_space=pl.ANY)
    dma = pltpu.SemaphoreType.DMA
    slots = pltpu.VMEM((planes, group, width), BF16)
    quads = pltpu.VMEM((PAIRS, EPG, group, width), BF16)
    return pl.pallas_call(
        functools.partial(expert_kernel, capacity),
        out_shape=jax.ShapeDtypeStruct((tok, width), BF16),
        in_specs=[vmem] * 4 + [hbm] * 5,
        out_specs=vmem,
        scratch_shapes=[
            pltpu.VMEM((tok, width), BF16),
            pltpu.VMEM(out_weight.shape, BF16),
            pltpu.VMEM(gate.shape, BF16),
            pltpu.VMEM(up.shape, BF16),
            pltpu.VMEM(down.shape, BF16),
            pltpu.VMEM((tok, width), F32),
            pltpu.VMEM((tok, width), BF16),
            slots, slots,
            pltpu.VMEM((planes, 16, 128), F32),
            pltpu.VMEM((planes, 16, 128), F32),
            pltpu.VMEM((planes, group, 128), F32),
            quads, quads, quads, quads,
            slots, slots,
            dma((5,)),
            dma((planes,)), dma((planes,)), dma((planes,)), dma((planes,)),
            dma((PAIRS, EPG)), dma((PAIRS, EPG)), dma((PAIRS, EPG)), dma((PAIRS, EPG)),
            dma((planes,)), dma((planes,)),
        ],
        compiler_params=pltpu.CompilerParams(
            collective_id=1, has_side_effects=True, vmem_limit_bytes=67043328
        ),
        name="experts",
    )(heads, norm_gain[None, :], expert_ids.T, route_weights.T, residual, out_weight, gate, up, down)


def per_device(
    query_rows,
    key_rows,
    value_rows,
    forget_cum,
    doc_ids,
    residual,
    out_weight,
    norm_gain,
    expert_ids,
    route_weights,
    gate_proj,
    up_proj,
    down_proj,
):
    heads = mixer(query_rows, key_rows, value_rows, forget_cum, doc_ids)
    return experts_layer(
        heads, residual, out_weight, norm_gain, expert_ids, route_weights, gate_proj[0], up_proj[0], down_proj[0]
    )


def solution(mesh):
    placed = (
        P("sp", "tp"),
        P("sp", "tp"),
        P("sp", "tp"),
        P("tp", "sp"),
        P("sp"),
        P(("sp", "tp"), None),
        P(),
        P(),
        P(("sp", "tp"), None),
        P(("sp", "tp"), None),
        P("sp", None, None),
        P("sp", None, None),
        P("sp", None, None),
    )
    return jax.shard_map(
        per_device, mesh=mesh, in_specs=placed, out_specs=P(("sp", "tp"), None), check_vma=False
    )
```

```python
import functools
import jax
import jax.numpy as jnp
from jax import lax
from jax.experimental import pallas as pl
from jax.experimental.pallas import tpu as pltpu
from jax.sharding import PartitionSpec as P

EPG = 4
TOPK = 2
REACH = 3
QT = 512
QF = 1024
KT = 512
FAR = -1e30
CUTS = 2
STRAIGHT = ()

norm_eps = 1e-06
F32 = jnp.float32
BF16 = jnp.bfloat16


def columns_of(rows):
    parts = [jnp.transpose(rows[:, c : c + 128]) for c in range(0, rows.shape[1], 128)]
    return jnp.concatenate(parts, axis=0).astype(BF16)


def mixer_kernel(
    n_sp, n_tp, q_hbm, k_hbm, v_hbm, gate_ref, doc_ref, out_ref,
    q_ref, k_ref, v_ref, marks_ref, krel, vrel, mrel,
    kbuf, vbuf, mbuf, qaug, keyt, vaug, top, acc, att, heads,
    load, rsend, rrecv, hsend, hrecv, asend, arecv,
):
    sp = lax.axis_index("sp")
    tp = lax.axis_index("tp")
    tok = q_ref.shape[0]
    chunk = tok // n_tp

    x = lax.rem(sp, EPG)
    z = sp // EPG
    planes = n_sp // EPG

    def along_x(hop):
        return {"sp": z * EPG + lax.rem(x + hop, EPG)}

    def along_z(hop):
        return {"sp": lax.rem(z + hop, planes) * EPG + x}

    barrier = pltpu.get_barrier_semaphore()
    for hop in range(1, EPG):
        pl.semaphore_signal(barrier, inc=1, device_id=along_x(hop))
    for hop in (1, planes - 1):
        pl.semaphore_signal(barrier, inc=1, device_id=along_z(hop))
    for d in range(1, REACH + 1):
        for other in (lax.rem(sp + d, n_sp), lax.rem(sp + n_sp - d, n_sp)):
            pl.semaphore_signal(barrier, inc=1, device_id={"sp": other})
    for d in range(1, n_tp):
        pl.semaphore_signal(barrier, inc=1, device_id={"tp": lax.rem(tp + d, n_tp)})

    loads = [
        pltpu.make_async_copy(src, dst, load.at[i])
        for i, (src, dst) in enumerate(((k_hbm, k_ref), (v_hbm, v_ref), (q_hbm, q_ref)))
    ]
    for copy in loads:
        copy.start()
    marks_ref[...] = jnp.concatenate(
        [gate_ref[...], doc_ref[...].astype(F32), jnp.zeros((5, tok), F32)], axis=0
    )
    pl.semaphore_wait(barrier, EPG - 1 + 2 + 2 * REACH + n_tp - 1)

    part = tok // CUTS
    pieces = [(marks_ref, mrel, mbuf, None)]
    for src, rel, buf in ((k_ref, krel, kbuf), (v_ref, vrel, vbuf)):
        pieces += [(src, rel, buf, pl.ds(c * part, part)) for c in range(CUTS)]

    def across(i):
        src, rel, buf, rows = pieces[i]
        if rows is not None:
            src, rel = src.at[rows], rel.at[rows]
        return pltpu.make_async_remote_copy(
            src_ref=src, dst_ref=rel, send_sem=rsend.at[i], recv_sem=rrecv.at[i], device_id=along_z(1)
        )

    def along(i, d, relayed):
        src, rel, buf, rows = pieces[i]
        src = rel if relayed else src
        dst = buf.at[d - 1]
        if rows is not None:
            src, dst = src.at[rows], dst.at[rows]
        return pltpu.make_async_remote_copy(
            src_ref=src, dst_ref=dst, send_sem=hsend.at[d - 1, i], recv_sem=hrecv.at[d - 1, i],
            device_id=along_x(d) if relayed else {"sp": lax.rem(sp + d, n_sp)},
        )

    def straight(d):
        here = x + d < EPG
        for column, far in STRAIGHT:
            if far == d:
                here = here | (x == column)
        return here

    relays = sorted({c for c in range(1, EPG) for d in range(EPG - c, EPG) if (c, d) not in STRAIGHT})

    def relaying():
        here = x == relays[0]
        for c in relays[1:]:
            here = here | (x == c)
        return here

    for i in range(len(pieces)):
        if i in (1, 1 + CUTS):
            loads[0 if i == 1 else 1].wait()

        @pl.when(relaying())
        def _(i=i):
            across(i).start()

        for d in range(1, REACH + 1):

            @pl.when(straight(d))
            def _(i=i, d=d):
                along(i, d, False).start()

    loads[2].wait()

    def pass_on(i):
        @pl.when(relaying())
        def _():
            across(i).wait_recv()

        for d in range(1, REACH + 1):

            @pl.when(jnp.logical_not(straight(d)))
            def _(d=d):
                along(i, d, True).start()

    lane = lax.broadcasted_iota(jnp.int32, (1, 128), 1)
    row8 = lax.broadcasted_iota(jnp.int32, (8, tok), 0)
    row16 = lax.broadcasted_iota(jnp.int32, (16, tok), 0).astype(F32)
    blank = jnp.zeros((104, tok), F32)
    own = marks_ref[...]
    base = own[0:2, 0:1]

    same = (own[2:3, :] == row16).astype(F32)
    qmark = columns_of(jnp.concatenate([jnp.zeros((8, tok), F32), same, blank], axis=0))
    qrows = q_ref[...] * jnp.asarray(0.125, BF16)
    for h in range(2):
        mine = (lane >= 64 * h) & (lane < 64 * h + 64)
        ones = (lane >= 3 * h) & (lane < 3 * h + 3)
        qaug[h, :, 0:128] = jnp.where(mine, qrows, jnp.zeros_like(qrows))
        qaug[h, :, 128:256] = jnp.where(ones, jnp.ones_like(qmark), qmark)

    def prepare(marks, keys, v):
        gate = base - marks[0:2, :]
        high = gate.astype(BF16).astype(F32)
        rest = gate - high
        mid = rest.astype(BF16).astype(F32)
        low = rest - mid
        pieces = jnp.zeros((8, tok), F32)
        for h in range(2):
            for i, piece in enumerate((high, mid, low)):
                pieces = jnp.where(row8 == 3 * h + i, piece[h : h + 1, :], pieces)
        other = jnp.where(marks[2:3, :] == row16, 0.0, FAR).astype(F32)
        keyt[128:256, :] = jnp.concatenate([pieces, other, blank], axis=0).astype(BF16)
        for c in range(0, tok, 128):
            keyt[0:128, c : c + 128] = jnp.transpose(keys[c : c + 128, :].astype(F32)).astype(BF16)
        one = jnp.ones_like(v)
        vaug[0] = jnp.where(lane < 64, v, one)
        vaug[1] = jnp.where(lane < 64, one, v)

    def tile(q0, k0, fresh, causal, wide=QT):
        rows = pl.ds(q0, wide)
        for h in range(2):
            score = jnp.dot(qaug[h, rows, :], keyt[:, pl.ds(k0, KT)], preferred_element_type=F32)
            if causal:
                qpos = q0 + lax.broadcasted_iota(jnp.int32, (wide, KT), 0)
                kpos = k0 + lax.broadcasted_iota(jnp.int32, (wide, KT), 1)
                score = jnp.where(kpos <= qpos, score, FAR)
            best = jnp.broadcast_to(jnp.max(score, axis=1, keepdims=True), (wide, 128))
            if not fresh:
                old = top[h, rows, :]
                best = jnp.maximum(best, old)
            expo = jnp.exp(score - jnp.concatenate([best] * (KT // 128), axis=1)).astype(BF16)
            part = jnp.dot(expo, vaug[h, pl.ds(k0, KT), :], preferred_element_type=F32)
            if not fresh:
                part = acc[h, rows, :] * jnp.exp(old - best) + part
            top[h, rows, :] = best
            acc[h, rows, :] = part

    prepare(own, k_ref, v_ref[...])
    tiles = tok // QT
    per = KT // QT
    for k0 in range(0, tok, KT):
        first = k0 // QT

        def diagonal(i, carry, k0=k0):
            tile(pl.multiple_of(i * QT, QT), k0, k0 == 0, True)
            return carry

        def below(i, carry, k0=k0):
            tile(pl.multiple_of(i * QT, QT), k0, k0 == 0, False)
            return carry

        lax.fori_loop(first, first + per, diagonal, 0)
        if first + per < tiles:
            lax.fori_loop(first + per, tiles, below, 0)

    for i in range(len(pieces)):
        pass_on(i)
    for d in range(1, REACH + 1):
        for i in range(len(pieces)):
            along(i, d, False).wait_recv()
        prepare(mbuf[d - 1], kbuf.at[d - 1], vbuf[d - 1])
        if d < REACH:

            def full(i, carry):
                for k0 in range(0, tok, KT):
                    tile(pl.multiple_of(i * QF, QF), k0, False, False, QF)
                return carry

            lax.fori_loop(0, tok // QF, full, 0)

    for i in range(tiles):
        q0 = i * QT
        for k0 in range(q0 // KT * KT, tok, KT):
            tile(q0, k0, False, False)
        rows = pl.ds(q0, QT)
        total = jnp.where(lane < 64, pltpu.roll(acc[0, rows, :], 64, 1), pltpu.roll(acc[1, rows, :], 64, 1))
        value = jnp.where(lane < 64, acc[0, rows, :], acc[1, rows, :])
        att[rows, :] = (value / total).astype(BF16)
        for c in range(q0 // chunk, (q0 + QT) // chunk):

            @pl.when(tp != c)
            def _(c=c):
                pltpu.make_async_remote_copy(
                    src_ref=att.at[pl.ds(c * chunk, chunk)], dst_ref=heads.at[tp],
                    send_sem=asend.at[c], recv_sem=arecv.at[tp], device_id={"tp": c},
                ).start()

    for c in range(n_tp):

        @pl.when(tp != c)
        def _(c=c):
            pltpu.make_async_remote_copy(
                src_ref=att.at[pl.ds(c * chunk, chunk)], dst_ref=heads.at[c],
                send_sem=asend.at[c], recv_sem=arecv.at[c], device_id={"tp": c},
            ).wait_recv()
            out_ref[:, c * 128 : (c + 1) * 128] = heads[c]

        @pl.when(tp == c)
        def _(c=c):
            out_ref[:, c * 128 : (c + 1) * 128] = att[c * chunk : (c + 1) * chunk, :]

    for c in range(n_tp):

        @pl.when(tp != c)
        def _(c=c):
            pltpu.make_async_remote_copy(
                src_ref=att.at[pl.ds(c * chunk, chunk)], dst_ref=heads.at[c],
                send_sem=asend.at[c], recv_sem=arecv.at[c], device_id={"tp": c},
            ).wait_send()

    for i in range(len(pieces)):

        @pl.when(relaying())
        def _(i=i):
            across(i).wait_send()

        for d in range(1, REACH + 1):
            along(i, d, False).wait_send()


def mixer(query_rows, key_rows, value_rows, forget_cum, doc_ids):
    n_sp, n_tp = lax.axis_size("sp"), lax.axis_size("tp")
    tok, width = query_rows.shape
    vmem = pl.BlockSpec(memory_space=pltpu.VMEM)
    hbm = pl.BlockSpec(memory_space=pl.ANY)
    dma = pltpu.SemaphoreType.DMA
    return pl.pallas_call(
        functools.partial(mixer_kernel, n_sp, n_tp),
        out_shape=jax.ShapeDtypeStruct((tok // n_tp, width * n_tp), BF16),
        in_specs=[hbm] * 3 + [vmem] * 2,
        out_specs=vmem,
        scratch_shapes=[
            pltpu.VMEM((tok, width), BF16),
            pltpu.VMEM((tok, width), BF16),
            pltpu.VMEM((tok, width), BF16),
            pltpu.VMEM((8, tok), F32),
            pltpu.VMEM((tok, width), BF16),
            pltpu.VMEM((tok, width), BF16),
            pltpu.VMEM((8, tok), F32),
            pltpu.VMEM((REACH, tok, width), BF16),
            pltpu.VMEM((REACH, tok, width), BF16),
            pltpu.VMEM((REACH, 8, tok), F32),
            pltpu.VMEM((2, tok, 2 * width), BF16),
            pltpu.VMEM((2 * width, tok), BF16),
            pltpu.VMEM((2, tok, width), BF16),
            pltpu.VMEM((2, tok, 128), F32),
            pltpu.VMEM((2, tok, 128), F32),
            pltpu.VMEM((tok, width), BF16),
            pltpu.VMEM((n_tp, tok // n_tp, width), BF16),
            dma((3,)),
            dma((1 + 2 * CUTS,)), dma((1 + 2 * CUTS,)),
            dma((REACH, 1 + 2 * CUTS)), dma((REACH, 1 + 2 * CUTS)),
            dma((n_tp,)), dma((n_tp,)),
        ],
        compiler_params=pltpu.CompilerParams(
            collective_id=0, has_side_effects=True, vmem_limit_bytes=67043328
        ),
        name="mixer",
    )(query_rows, key_rows, value_rows, forget_cum, doc_ids[None, :])


HOPS = (2, 6, 3, 5, 4, 0, 1, 7)
PAIRS = len(HOPS) // 2
HERE = HOPS.index(0)
AWAY = [s for s in range(len(HOPS)) if s != HERE]


def stack(blocks):
    parts = []
    for block in blocks:
        parts += [block.astype(F32), jnp.zeros((64 - block.shape[0], block.shape[1]), F32)]
    return jnp.concatenate(parts, axis=0).astype(BF16)


def expert_kernel(
    capacity, heads_ref, gain_ref, ids_ref, weights_ref, residual_hbm, mix_hbm, gate_hbm, up_hbm, down_hbm, out_ref,
    residual_ref, mix, wgate, wup, wdown, hidden, normed, zs, zbuf, ms, mbuf, mcol, xs, xbuf, ys, ybuf, cs, cbuf,
    load, zsend, zrecv, msend, mrecv, xsend, xrecv, ysend, yrecv, csend, crecv,
):
    sp = lax.axis_index("sp")
    x = lax.rem(sp, EPG)
    z = sp // EPG
    planes = len(HOPS)
    group = 2 * capacity
    tok, width = residual_ref.shape
    ffe = wgate.shape[1]

    def along_z(hop):
        return {"sp": lax.rem(z + hop, planes) * EPG + x}

    def along_x(hop):
        return {"sp": z * EPG + lax.rem(x + hop, EPG)}

    barrier = pltpu.get_barrier_semaphore()
    for hop in range(1, planes):
        pl.semaphore_signal(barrier, inc=1, device_id=along_z(hop))
    for hop in range(1, EPG):
        pl.semaphore_signal(barrier, inc=1, device_id=along_x(hop))

    loads = [
        pltpu.make_async_copy(src, dst, load.at[i])
        for i, (src, dst) in enumerate(
            ((residual_hbm, residual_ref), (mix_hbm, mix), (gate_hbm, wgate), (up_hbm, wup), (down_hbm, wdown))
        )
    ]
    for copy in loads:
        copy.start()

    ids = ids_ref[...]
    id0, id1 = ids[0:1, :], ids[1:2, :]
    earlier = (
        lax.broadcasted_iota(jnp.int32, (tok, tok), 0) < lax.broadcasted_iota(jnp.int32, (tok, tok), 1)
    ).astype(BF16)
    number = lax.broadcasted_iota(jnp.int32, (planes * EPG, tok), 0)
    uses = ((number == id0) | (number == id1)).astype(F32)
    rank = jnp.dot(uses.astype(BF16), earlier, preferred_element_type=F32)
    row = lax.broadcasted_iota(jnp.int32, (16, tok), 0)
    which = lax.rem(x + row, EPG)
    pick = (
        (lax.broadcasted_iota(jnp.int32, (16, planes * EPG), 1) & (EPG - 1))
        == lax.rem(x + lax.broadcasted_iota(jnp.int32, (16, planes * EPG), 0), EPG)
    ).astype(BF16)
    slots = jnp.dot(pick, (uses * (rank + 1.0)).astype(BF16), preferred_element_type=F32)
    weight = jnp.where((id0 & (EPG - 1)) == which, weights_ref[0:1, :], 0.0) + jnp.where(
        (id1 & (EPG - 1)) == which, weights_ref[1:2, :], 0.0
    )
    high = weight.astype(BF16).astype(F32)
    info = jnp.where(row < 4, slots, jnp.where(row < 8, high, jnp.where(row < 12, weight - high, 0.0)))
    info = info.astype(BF16)
    mine = lax.shift_right_logical(id0, 2)
    member = (lax.broadcasted_iota(jnp.int32, (planes, tok), 0) == mine).astype(F32)
    place = jnp.sum(
        member * jnp.dot(member.astype(BF16), earlier, preferred_element_type=F32), axis=0, keepdims=True
    )
    mine = mine.astype(F32)
    spot = lax.broadcasted_iota(jnp.int32, (group, tok), 0).astype(F32)
    sel = []
    for hop in HOPS:
        there = lax.rem(z + hop, planes).astype(F32)
        sel.append(jnp.where((mine == there) & (place == spot), 1.0, 0.0))
    for s in range(planes):
        table = lax.dot_general(
            info, sel[s].astype(BF16), (((1,), (1,)), ((), ())), preferred_element_type=F32
        )
        rest = jnp.zeros((16, 64 - group), F32)
        table = [table, rest, jnp.zeros((16, 64), F32)] if s % 2 == 0 else [jnp.zeros((16, 64), F32), table, rest]
        table = jnp.concatenate(table, axis=1)
        if s == HERE:
            mbuf[s] = table
        else:
            ms[s] = table
    sel = jnp.concatenate(sel, axis=0).astype(BF16)
    wide = lax.broadcasted_iota(jnp.int32, (tok, tok), 0)
    cols = jnp.transpose(jnp.where(wide == 0, mine, jnp.where(wide == 1, place, 0.0)))

    loads[0].wait()
    loads[1].wait()
    square = jnp.zeros((tok, 128), F32)
    for c in range(0, width, 512):
        part = jnp.dot(heads_ref[...], mix[:, c : c + 512], preferred_element_type=F32)
        part = part + residual_ref[:, c : c + 512].astype(F32)
        hidden[:, c : c + 512] = part
        for i in range(0, 512, 128):
            square = square + part[:, i : i + 128] * part[:, i : i + 128]
    scale = lax.rsqrt(jnp.sum(square, axis=1, keepdims=True) / width + norm_eps)
    for c in range(0, width, 512):
        normed[:, c : c + 512] = (
            hidden[:, c : c + 512] * scale * gain_ref[:, c : c + 512]
        ).astype(BF16)

    for c in range(0, width, 512):
        part = jnp.dot(sel, normed[:, c : c + 512], preferred_element_type=F32)
        for s in range(planes):
            into = zbuf if s == HERE else zs
            into[s, :, c : c + 512] = part[s * group : (s + 1) * group].astype(BF16)
    pl.semaphore_wait(barrier, planes + EPG - 2)

    def zcopy(s):
        return pltpu.make_async_remote_copy(
            src_ref=zs.at[s], dst_ref=zbuf.at[s], send_sem=zsend.at[s], recv_sem=zrecv.at[s],
            device_id=along_z(HOPS[s]),
        )

    def mcopy(s):
        return pltpu.make_async_remote_copy(
            src_ref=ms.at[s], dst_ref=mbuf.at[s], send_sem=msend.at[s], recv_sem=mrecv.at[s],
            device_id=along_z(HOPS[s]),
        )

    def xcopy(p, hop):
        return pltpu.make_async_remote_copy(
            src_ref=xs.at[p, hop], dst_ref=xbuf.at[p, hop], send_sem=xsend.at[p, hop],
            recv_sem=xrecv.at[p, hop], device_id=along_x(hop),
        )

    def ycopy(p, hop):
        return pltpu.make_async_remote_copy(
            src_ref=ys.at[p, hop], dst_ref=ybuf.at[p, hop], send_sem=ysend.at[p, hop],
            recv_sem=yrecv.at[p, hop], device_id=along_x(EPG - hop),
        )

    def ccopy(s):
        return pltpu.make_async_remote_copy(
            src_ref=cs.at[s], dst_ref=cbuf.at[s], send_sem=csend.at[s], recv_sem=crecv.at[s],
            device_id=along_z(planes - HOPS[s]),
        )

    for s in AWAY:
        mcopy(s).start()
        zcopy(s).start()

    def spread(p):
        for half in range(2):
            s = 2 * p + half
            if s != HERE:
                mcopy(s).wait_recv()
            table = jnp.concatenate([mbuf[s], jnp.zeros((112, 128), F32)], axis=0)
            mcol[s] = jnp.transpose(table)[64 * half : 64 * half + group, :]
        second = mbuf[2 * p + 1]
        table = mbuf[2 * p] + jnp.where(second > 0.0, second + float(capacity), 0.0)
        want = lax.broadcasted_iota(jnp.int32, (group, 128), 0).astype(F32) + 1.0
        rows = [jnp.where(table[h : h + 1, :] == want, 1.0, 0.0) for h in range(EPG)]
        order = jnp.concatenate(rows, axis=0).astype(BF16)
        for half in range(2):
            if 2 * p + half != HERE:
                zcopy(2 * p + half).wait_recv()
        for c in range(0, width, 512):
            rows = stack([zbuf[2 * p, :, c : c + 512], zbuf[2 * p + 1, :, c : c + 512]])
            part = jnp.dot(order, rows, preferred_element_type=F32)
            xbuf[p, 0, :, c : c + 512] = part[0:group].astype(BF16)
            for h in range(1, EPG):
                xs[p, h, :, c : c + 512] = part[h * group : (h + 1) * group].astype(BF16)
        for h in range(1, EPG):
            xcopy(p, h).start()

    def expert(p):
        for h in range(1, EPG):
            xcopy(p, h).wait_recv()
        gate = jnp.zeros((EPG * group, ffe), F32)
        up = jnp.zeros((EPG * group, ffe), F32)
        for c in range(0, width, 512):
            rows = jnp.concatenate(
                [xbuf[p, h, :, c : c + 512].astype(F32) for h in range(EPG)], axis=0
            ).astype(BF16)
            gate = gate + jnp.dot(rows, wgate[c : c + 512, :], preferred_element_type=F32)
            up = up + jnp.dot(rows, wup[c : c + 512, :], preferred_element_type=F32)
        act = (gate / (1.0 + jnp.exp(-gate)) * up).astype(BF16)
        for c in range(0, width, 512):
            part = jnp.dot(act, wdown[:, c : c + 512], preferred_element_type=F32)
            ybuf[p, 0, :, c : c + 512] = part[0:group].astype(BF16)
            for h in range(1, EPG):
                ys[p, h, :, c : c + 512] = part[h * group : (h + 1) * group].astype(BF16)
        for h in range(1, EPG):
            ycopy(p, h).start()

    def collect(p):
        lanes = lax.broadcasted_iota(jnp.int32, (group, 128), 1)
        left = lanes < 64
        want = ((lanes & 63) + 1).astype(F32)
        mats = []
        for h in range(0, EPG, 2):
            parts = []
            for kind in (4, 8):
                for half in range(2):
                    col = mcol[2 * p + half]
                    goal = jnp.where(left, col[:, h : h + 1], col[:, h + 1 : h + 2])
                    goal = jnp.where(goal > 0.0, goal + float(half * capacity), 0.0)
                    share = jnp.where(left, col[:, kind + h : kind + h + 1], col[:, kind + h + 1 : kind + h + 2])
                    parts.append(jnp.where(goal == want, share, 0.0))
            mats.append(jnp.concatenate(parts, axis=0))
        mats = jnp.concatenate(mats, axis=1).astype(BF16)
        for h in range(1, EPG):
            ycopy(p, h).wait_recv()
        for c in range(0, width, 512):
            rows = stack([ybuf[p, h, :, c : c + 512] for h in range(EPG)])
            part = jnp.dot(mats, rows, preferred_element_type=F32)
            for half in range(2):
                both = part[half * group : (half + 1) * group] + part[(2 + half) * group : (3 + half) * group]
                s = 2 * p + half
                into = cbuf if s == HERE else cs
                into[s, :, c : c + 512] = both.astype(BF16)
        for half in range(2):
            if 2 * p + half != HERE:
                ccopy(2 * p + half).start()

    spread(0)
    for copy in loads[2:]:
        copy.wait()
    expert(0)
    spread(1)
    collect(0)
    expert(1)
    spread(2)
    spread(3)
    collect(1)
    expert(2)
    expert(3)
    collect(2)
    collect(3)

    lanes = lax.broadcasted_iota(jnp.int32, (tok, 128), 1)
    back = []
    for p in range(PAIRS):
        there = jnp.where(lanes < 64, lax.rem(z + HOPS[2 * p], planes), lax.rem(z + HOPS[2 * p + 1], planes))
        hit = (cols[:, 0:1] == there.astype(F32)) & (cols[:, 1:2] == (lanes & 63).astype(F32))
        back.append(jnp.where(hit, 1.0, 0.0))
    back = jnp.concatenate(back, axis=1).astype(BF16)
    for s in AWAY:
        ccopy(s).wait_recv()
    for c in range(0, width, 512):
        rows = stack([cbuf[s, :, c : c + 512] for s in range(planes)])
        part = jnp.dot(back, rows, preferred_element_type=F32)
        out_ref[:, c : c + 512] = hidden[:, c : c + 512] + part

    for s in AWAY:
        mcopy(s).wait_send()
        zcopy(s).wait_send()
        ccopy(s).wait_send()
    for p in range(PAIRS):
        for h in range(1, EPG):
            xcopy(p, h).wait_send()
            ycopy(p, h).wait_send()


def experts_layer(heads, residual, out_weight, norm_gain, expert_ids, route_weights, gate, up, down):
    tok, width = residual.shape
    ffe = gate.shape[1]
    planes = lax.axis_size("sp") // EPG
    capacity = max(2, 5 * tok // (4 * planes))
    group = 2 * capacity
    vmem = pl.BlockSpec(memory_space=pltpu.VMEM)
    hbm = pl.BlockSpec(memory_space=pl.ANY)
    dma = pltpu.SemaphoreType.DMA
    slots = pltpu.VMEM((planes, group, width), BF16)
    quads = pltpu.VMEM((PAIRS, EPG, group, width), BF16)
    return pl.pallas_call(
        functools.partial(expert_kernel, capacity),
        out_shape=jax.ShapeDtypeStruct((tok, width), F32),
        in_specs=[vmem] * 4 + [hbm] * 5,
        out_specs=vmem,
        scratch_shapes=[
            pltpu.VMEM((tok, width), BF16),
            pltpu.VMEM(out_weight.shape, BF16),
            pltpu.VMEM(gate.shape, BF16),
            pltpu.VMEM(up.shape, BF16),
            pltpu.VMEM(down.shape, BF16),
            pltpu.VMEM((tok, width), F32),
            pltpu.VMEM((tok, width), BF16),
            slots, slots,
            pltpu.VMEM((planes, 16, 128), F32),
            pltpu.VMEM((planes, 16, 128), F32),
            pltpu.VMEM((planes, group, 128), F32),
            quads, quads, quads, quads,
            slots, slots,
            dma((5,)),
            dma((planes,)), dma((planes,)), dma((planes,)), dma((planes,)),
            dma((PAIRS, EPG)), dma((PAIRS, EPG)), dma((PAIRS, EPG)), dma((PAIRS, EPG)),
            dma((planes,)), dma((planes,)),
        ],
        compiler_params=pltpu.CompilerParams(
            collective_id=1, has_side_effects=True, vmem_limit_bytes=67043328
        ),
        name="experts",
    )(heads, norm_gain[None, :], expert_ids.T, route_weights.T, residual, out_weight, gate, up, down).astype(BF16)


def per_device(
    query_rows,
    key_rows,
    value_rows,
    forget_cum,
    doc_ids,
    residual,
    out_weight,
    norm_gain,
    expert_ids,
    route_weights,
    gate_proj,
    up_proj,
    down_proj,
):
    heads = mixer(query_rows, key_rows, value_rows, forget_cum, doc_ids)
    return experts_layer(
        heads, residual, out_weight, norm_gain, expert_ids, route_weights, gate_proj[0], up_proj[0], down_proj[0]
    )


def solution(mesh):
    placed = (
        P("sp", "tp"),
        P("sp", "tp"),
        P("sp", "tp"),
        P("tp", "sp"),
        P("sp"),
        P(("sp", "tp"), None),
        P(),
        P(),
        P(("sp", "tp"), None),
        P(("sp", "tp"), None),
        P("sp", None, None),
        P("sp", None, None),
        P("sp", None, None),
    )
    return jax.shard_map(
        per_device, mesh=mesh, in_specs=placed, out_specs=P(("sp", "tp"), None), check_vma=False
    )
```

```python
import functools
import jax
import jax.numpy as jnp
from jax import lax
from jax.experimental import pallas as pl
from jax.experimental.pallas import tpu as pltpu
from jax.sharding import PartitionSpec as P

EPG = 4
TOPK = 2
REACH = 3
QT = 512
QF = 1024
KT = 512
FAR = -1e30
CUTS = 2

norm_eps = 1e-06
F32 = jnp.float32
BF16 = jnp.bfloat16


def columns_of(rows):
    parts = [jnp.transpose(rows[:, c : c + 128]) for c in range(0, rows.shape[1], 128)]
    return jnp.concatenate(parts, axis=0).astype(BF16)


def mix_heads(
    n_sp, n_tp, early, q_hbm, k_hbm, v_hbm, gate_ref, doc_ref, out_ref,
    q_ref, k_ref, v_ref, marks_ref, krel, vrel, mrel,
    kbuf, vbuf, mbuf, qaug, keyt, vaug, top, acc, att, heads,
    load, rsend, rrecv, hsend, hrecv, asend, arecv,
):
    sp = lax.axis_index("sp")
    tp = lax.axis_index("tp")
    tok = q_ref.shape[0]
    chunk = tok // n_tp

    x = lax.rem(sp, EPG)
    z = sp // EPG
    planes = n_sp // EPG

    def along_x(hop):
        return {"sp": z * EPG + lax.rem(x + hop, EPG)}

    def along_z(hop):
        return {"sp": lax.rem(z + hop, planes) * EPG + x}

    barrier = pltpu.get_barrier_semaphore()
    for hop in range(1, EPG):
        pl.semaphore_signal(barrier, inc=1, device_id=along_x(hop))
    for hop in range(1, planes):
        pl.semaphore_signal(barrier, inc=1, device_id=along_z(hop))
    for d in range(1, n_tp):
        pl.semaphore_signal(barrier, inc=1, device_id={"tp": lax.rem(tp + d, n_tp)})

    loads = [
        pltpu.make_async_copy(src, dst, load.at[i])
        for i, (src, dst) in enumerate(((k_hbm, k_ref), (v_hbm, v_ref), (q_hbm, q_ref)))
    ]
    for copy in loads:
        copy.start()
    marks_ref[...] = jnp.concatenate(
        [gate_ref[...], doc_ref[...].astype(F32), jnp.zeros((5, tok), F32)], axis=0
    )
    pl.semaphore_wait(barrier, EPG + planes - 2 + n_tp - 1)

    part = tok // CUTS
    pieces = [(marks_ref, mrel, mbuf, None)]
    for src, rel, buf in ((k_ref, krel, kbuf), (v_ref, vrel, vbuf)):
        pieces += [(src, rel, buf, pl.ds(c * part, part)) for c in range(CUTS)]

    def across(i):
        src, rel, buf, rows = pieces[i]
        if rows is not None:
            src, rel = src.at[rows], rel.at[rows]
        return pltpu.make_async_remote_copy(
            src_ref=src, dst_ref=rel, send_sem=rsend.at[i], recv_sem=rrecv.at[i], device_id=along_z(1)
        )

    def along(i, d, relayed):
        src, rel, buf, rows = pieces[i]
        src = rel if relayed else src
        dst = buf.at[d - 1]
        if rows is not None:
            src, dst = src.at[rows], dst.at[rows]
        return pltpu.make_async_remote_copy(
            src_ref=src, dst_ref=dst, send_sem=hsend.at[d - 1, i], recv_sem=hrecv.at[d - 1, i],
            device_id=along_x(d),
        )

    for i in range(len(pieces)):
        if i in (1, 1 + CUTS):
            loads[0 if i == 1 else 1].wait()

        @pl.when(x > 0)
        def _(i=i):
            across(i).start()

        for d in range(1, REACH + 1):

            @pl.when(x + d < EPG)
            def _(i=i, d=d):
                along(i, d, False).start()

    loads[2].wait()

    def pass_on(i):
        @pl.when(x > 0)
        def _():
            across(i).wait_recv()

        for d in range(1, REACH + 1):

            @pl.when(x + d >= EPG)
            def _(d=d):
                along(i, d, True).start()

    lane = lax.broadcasted_iota(jnp.int32, (1, 128), 1)
    row8 = lax.broadcasted_iota(jnp.int32, (8, tok), 0)
    row16 = lax.broadcasted_iota(jnp.int32, (16, tok), 0).astype(F32)
    blank = jnp.zeros((104, tok), F32)
    own = marks_ref[...]
    base = own[0:2, 0:1]

    same = (own[2:3, :] == row16).astype(F32)
    qmark = columns_of(jnp.concatenate([jnp.zeros((8, tok), F32), same, blank], axis=0))
    qrows = q_ref[...] * jnp.asarray(0.125, BF16)
    for h in range(2):
        mine = (lane >= 64 * h) & (lane < 64 * h + 64)
        ones = (lane >= 3 * h) & (lane < 3 * h + 3)
        qaug[h, :, 0:128] = jnp.where(mine, qrows, jnp.zeros_like(qrows))
        qaug[h, :, 128:256] = jnp.where(ones, jnp.ones_like(qmark), qmark)

    def prepare(marks, keys, v):
        gate = base - marks[0:2, :]
        high = gate.astype(BF16).astype(F32)
        rest = gate - high
        mid = rest.astype(BF16).astype(F32)
        low = rest - mid
        pieces = jnp.zeros((8, tok), F32)
        for h in range(2):
            for i, piece in enumerate((high, mid, low)):
                pieces = jnp.where(row8 == 3 * h + i, piece[h : h + 1, :], pieces)
        other = jnp.where(marks[2:3, :] == row16, 0.0, FAR).astype(F32)
        keyt[128:256, :] = jnp.concatenate([pieces, other, blank], axis=0).astype(BF16)
        for c in range(0, tok, 128):
            keyt[0:128, c : c + 128] = jnp.transpose(keys[c : c + 128, :].astype(F32)).astype(BF16)
        one = jnp.ones_like(v)
        vaug[0] = jnp.where(lane < 64, v, one)
        vaug[1] = jnp.where(lane < 64, one, v)

    def tile(q0, k0, fresh, causal, wide=QT):
        rows = pl.ds(q0, wide)
        for h in range(2):
            score = jnp.dot(qaug[h, rows, :], keyt[:, pl.ds(k0, KT)], preferred_element_type=F32)
            if causal:
                qpos = q0 + lax.broadcasted_iota(jnp.int32, (wide, KT), 0)
                kpos = k0 + lax.broadcasted_iota(jnp.int32, (wide, KT), 1)
                score = jnp.where(kpos <= qpos, score, FAR)
            best = jnp.broadcast_to(jnp.max(score, axis=1, keepdims=True), (wide, 128))
            if not fresh:
                old = top[h, rows, :]
                best = jnp.maximum(best, old)
            expo = jnp.exp(score - jnp.concatenate([best] * (KT // 128), axis=1)).astype(BF16)
            part = jnp.dot(expo, vaug[h, pl.ds(k0, KT), :], preferred_element_type=F32)
            if not fresh:
                part = acc[h, rows, :] * jnp.exp(old - best) + part
            top[h, rows, :] = best
            acc[h, rows, :] = part

    prepare(own, k_ref, v_ref[...])
    tiles = tok // QT
    per = KT // QT
    for k0 in range(0, tok, KT):
        first = k0 // QT

        def diagonal(i, carry, k0=k0):
            tile(pl.multiple_of(i * QT, QT), k0, k0 == 0, True)
            return carry

        def below(i, carry, k0=k0):
            tile(pl.multiple_of(i * QT, QT), k0, k0 == 0, False)
            return carry

        lax.fori_loop(first, first + per, diagonal, 0)
        if first + per < tiles:
            lax.fori_loop(first + per, tiles, below, 0)

    early()
    for i in range(len(pieces)):
        pass_on(i)
    for d in range(1, REACH + 1):
        for i in range(len(pieces)):
            along(i, d, False).wait_recv()
        prepare(mbuf[d - 1], kbuf.at[d - 1], vbuf[d - 1])
        if d < REACH:

            def full(i, carry):
                for k0 in range(0, tok, KT):
                    tile(pl.multiple_of(i * QF, QF), k0, False, False, QF)
                return carry

            lax.fori_loop(0, tok // QF, full, 0)

    for i in range(tiles):
        q0 = i * QT
        for k0 in range(q0 // KT * KT, tok, KT):
            tile(q0, k0, False, False)
        rows = pl.ds(q0, QT)
        total = jnp.where(lane < 64, pltpu.roll(acc[0, rows, :], 64, 1), pltpu.roll(acc[1, rows, :], 64, 1))
        value = jnp.where(lane < 64, acc[0, rows, :], acc[1, rows, :])
        att[rows, :] = (value / total).astype(BF16)
        for c in range(q0 // chunk, (q0 + QT) // chunk):

            @pl.when(tp != c)
            def _(c=c):
                pltpu.make_async_remote_copy(
                    src_ref=att.at[pl.ds(c * chunk, chunk)], dst_ref=heads.at[tp],
                    send_sem=asend.at[c], recv_sem=arecv.at[tp], device_id={"tp": c},
                ).start()

    for c in range(n_tp):

        @pl.when(tp != c)
        def _(c=c):
            pltpu.make_async_remote_copy(
                src_ref=att.at[pl.ds(c * chunk, chunk)], dst_ref=heads.at[c],
                send_sem=asend.at[c], recv_sem=arecv.at[c], device_id={"tp": c},
            ).wait_recv()
            out_ref[:, c * 128 : (c + 1) * 128] = heads[c]

        @pl.when(tp == c)
        def _(c=c):
            out_ref[:, c * 128 : (c + 1) * 128] = att[c * chunk : (c + 1) * chunk, :]

    def drain():
        for c in range(n_tp):

            @pl.when(tp != c)
            def _(c=c):
                pltpu.make_async_remote_copy(
                    src_ref=att.at[pl.ds(c * chunk, chunk)], dst_ref=heads.at[c],
                    send_sem=asend.at[c], recv_sem=arecv.at[c], device_id={"tp": c},
                ).wait_send()

        for i in range(len(pieces)):

            @pl.when(x > 0)
            def _(i=i):
                across(i).wait_send()

            for d in range(1, REACH + 1):
                along(i, d, False).wait_send()

    return drain


HOPS = (2, 6, 3, 5, 4, 0, 1, 7)
PAIRS = len(HOPS) // 2
HERE = HOPS.index(0)
AWAY = [s for s in range(len(HOPS)) if s != HERE]


def stack(blocks):
    parts = []
    for block in blocks:
        parts += [block.astype(F32), jnp.zeros((64 - block.shape[0], block.shape[1]), F32)]
    return jnp.concatenate(parts, axis=0).astype(BF16)


def route_and_run(
    capacity, heads_ref, gain_ref, ids_ref, weights_ref, residual_hbm, mix_hbm, gate_hbm, up_hbm, down_hbm, out_ref,
    residual_ref, mix, wgate, wup, wdown, hidden, normed, zs, zbuf, ms, mbuf, mcol, xs, xbuf, ys, ybuf, cs, cbuf,
    load, zsend, zrecv, msend, mrecv, xsend, xrecv, ysend, yrecv, csend, crecv,
):
    sp = lax.axis_index("sp")
    x = lax.rem(sp, EPG)
    z = sp // EPG
    planes = len(HOPS)
    group = 2 * capacity
    tok, width = residual_ref.shape
    ffe = wgate.shape[1]

    def along_z(hop):
        return {"sp": lax.rem(z + hop, planes) * EPG + x}

    def along_x(hop):
        return {"sp": z * EPG + lax.rem(x + hop, EPG)}

    loads = [
        pltpu.make_async_copy(src, dst, load.at[i])
        for i, (src, dst) in enumerate(
            ((residual_hbm, residual_ref), (mix_hbm, mix), (gate_hbm, wgate), (up_hbm, wup), (down_hbm, wdown))
        )
    ]
    for copy in loads:
        copy.start()

    ids = ids_ref[...]
    id0, id1 = ids[0:1, :], ids[1:2, :]
    earlier = (
        lax.broadcasted_iota(jnp.int32, (tok, tok), 0) < lax.broadcasted_iota(jnp.int32, (tok, tok), 1)
    ).astype(BF16)
    number = lax.broadcasted_iota(jnp.int32, (planes * EPG, tok), 0)
    uses = ((number == id0) | (number == id1)).astype(F32)
    rank = jnp.dot(uses.astype(BF16), earlier, preferred_element_type=F32)
    row = lax.broadcasted_iota(jnp.int32, (16, tok), 0)
    which = lax.rem(x + row, EPG)
    pick = (
        (lax.broadcasted_iota(jnp.int32, (16, planes * EPG), 1) & (EPG - 1))
        == lax.rem(x + lax.broadcasted_iota(jnp.int32, (16, planes * EPG), 0), EPG)
    ).astype(BF16)
    slots = jnp.dot(pick, (uses * (rank + 1.0)).astype(BF16), preferred_element_type=F32)
    weight = jnp.where((id0 & (EPG - 1)) == which, weights_ref[0:1, :], 0.0) + jnp.where(
        (id1 & (EPG - 1)) == which, weights_ref[1:2, :], 0.0
    )
    high = weight.astype(BF16).astype(F32)
    info = jnp.where(row < 4, slots, jnp.where(row < 8, high, jnp.where(row < 12, weight - high, 0.0)))
    info = info.astype(BF16)
    mine = lax.shift_right_logical(id0, 2)
    member = (lax.broadcasted_iota(jnp.int32, (planes, tok), 0) == mine).astype(F32)
    place = jnp.sum(
        member * jnp.dot(member.astype(BF16), earlier, preferred_element_type=F32), axis=0, keepdims=True
    )
    mine = mine.astype(F32)
    spot = lax.broadcasted_iota(jnp.int32, (group, tok), 0).astype(F32)
    sel = []
    for hop in HOPS:
        there = lax.rem(z + hop, planes).astype(F32)
        sel.append(jnp.where((mine == there) & (place == spot), 1.0, 0.0))
    for s in range(planes):
        table = lax.dot_general(
            info, sel[s].astype(BF16), (((1,), (1,)), ((), ())), preferred_element_type=F32
        )
        rest = jnp.zeros((16, 64 - group), F32)
        table = [table, rest, jnp.zeros((16, 64), F32)] if s % 2 == 0 else [jnp.zeros((16, 64), F32), table, rest]
        table = jnp.concatenate(table, axis=1)
        if s == HERE:
            mbuf[s] = table
        else:
            ms[s] = table
    sel = jnp.concatenate(sel, axis=0).astype(BF16)
    wide = lax.broadcasted_iota(jnp.int32, (tok, tok), 0)
    cols = jnp.transpose(jnp.where(wide == 0, mine, jnp.where(wide == 1, place, 0.0)))

    yield

    loads[0].wait()
    loads[1].wait()
    square = jnp.zeros((tok, 128), F32)
    for c in range(0, width, 512):
        part = jnp.dot(heads_ref[...], mix[:, c : c + 512], preferred_element_type=F32)
        part = part + residual_ref[:, c : c + 512].astype(F32)
        hidden[:, c : c + 512] = part
        for i in range(0, 512, 128):
            square = square + part[:, i : i + 128] * part[:, i : i + 128]
    scale = lax.rsqrt(jnp.sum(square, axis=1, keepdims=True) / width + norm_eps)
    for c in range(0, width, 512):
        normed[:, c : c + 512] = (
            hidden[:, c : c + 512] * scale * gain_ref[:, c : c + 512]
        ).astype(BF16)

    for c in range(0, width, 512):
        part = jnp.dot(sel, normed[:, c : c + 512], preferred_element_type=F32)
        for s in range(planes):
            into = zbuf if s == HERE else zs
            into[s, :, c : c + 512] = part[s * group : (s + 1) * group].astype(BF16)

    def zcopy(s):
        return pltpu.make_async_remote_copy(
            src_ref=zs.at[s], dst_ref=zbuf.at[s], send_sem=zsend.at[s], recv_sem=zrecv.at[s],
            device_id=along_z(HOPS[s]),
        )

    def mcopy(s):
        return pltpu.make_async_remote_copy(
            src_ref=ms.at[s], dst_ref=mbuf.at[s], send_sem=msend.at[s], recv_sem=mrecv.at[s],
            device_id=along_z(HOPS[s]),
        )

    def xcopy(p, hop):
        return pltpu.make_async_remote_copy(
            src_ref=xs.at[p, hop], dst_ref=xbuf.at[p, hop], send_sem=xsend.at[p, hop],
            recv_sem=xrecv.at[p, hop], device_id=along_x(hop),
        )

    def ycopy(p, hop):
        return pltpu.make_async_remote_copy(
            src_ref=ys.at[p, hop], dst_ref=ybuf.at[p, hop], send_sem=ysend.at[p, hop],
            recv_sem=yrecv.at[p, hop], device_id=along_x(EPG - hop),
        )

    def ccopy(s):
        return pltpu.make_async_remote_copy(
            src_ref=cs.at[s], dst_ref=cbuf.at[s], send_sem=csend.at[s], recv_sem=crecv.at[s],
            device_id=along_z(planes - HOPS[s]),
        )

    for s in AWAY:
        mcopy(s).start()
        zcopy(s).start()

    def spread(p):
        for half in range(2):
            s = 2 * p + half
            if s != HERE:
                mcopy(s).wait_recv()
            table = jnp.concatenate([mbuf[s], jnp.zeros((112, 128), F32)], axis=0)
            mcol[s] = jnp.transpose(table)[64 * half : 64 * half + group, :]
        second = mbuf[2 * p + 1]
        table = mbuf[2 * p] + jnp.where(second > 0.0, second + float(capacity), 0.0)
        want = lax.broadcasted_iota(jnp.int32, (group, 128), 0).astype(F32) + 1.0
        rows = [jnp.where(table[h : h + 1, :] == want, 1.0, 0.0) for h in range(EPG)]
        order = jnp.concatenate(rows, axis=0).astype(BF16)
        for half in range(2):
            if 2 * p + half != HERE:
                zcopy(2 * p + half).wait_recv()
        for c in range(0, width, 512):
            rows = stack([zbuf[2 * p, :, c : c + 512], zbuf[2 * p + 1, :, c : c + 512]])
            part = jnp.dot(order, rows, preferred_element_type=F32)
            xbuf[p, 0, :, c : c + 512] = part[0:group].astype(BF16)
            for h in range(1, EPG):
                xs[p, h, :, c : c + 512] = part[h * group : (h + 1) * group].astype(BF16)
        for h in range(1, EPG):
            xcopy(p, h).start()

    def expert(p):
        for h in range(1, EPG):
            xcopy(p, h).wait_recv()
        gate = jnp.zeros((EPG * group, ffe), F32)
        up = jnp.zeros((EPG * group, ffe), F32)
        for c in range(0, width, 512):
            rows = jnp.concatenate(
                [xbuf[p, h, :, c : c + 512].astype(F32) for h in range(EPG)], axis=0
            ).astype(BF16)
            gate = gate + jnp.dot(rows, wgate[c : c + 512, :], preferred_element_type=F32)
            up = up + jnp.dot(rows, wup[c : c + 512, :], preferred_element_type=F32)
        act = (gate / (1.0 + jnp.exp(-gate)) * up).astype(BF16)
        for c in range(0, width, 512):
            part = jnp.dot(act, wdown[:, c : c + 512], preferred_element_type=F32)
            ybuf[p, 0, :, c : c + 512] = part[0:group].astype(BF16)
            for h in range(1, EPG):
                ys[p, h, :, c : c + 512] = part[h * group : (h + 1) * group].astype(BF16)
        for h in range(1, EPG):
            ycopy(p, h).start()

    def collect(p):
        lanes = lax.broadcasted_iota(jnp.int32, (group, 128), 1)
        left = lanes < 64
        want = ((lanes & 63) + 1).astype(F32)
        mats = []
        for h in range(0, EPG, 2):
            parts = []
            for kind in (4, 8):
                for half in range(2):
                    col = mcol[2 * p + half]
                    goal = jnp.where(left, col[:, h : h + 1], col[:, h + 1 : h + 2])
                    goal = jnp.where(goal > 0.0, goal + float(half * capacity), 0.0)
                    share = jnp.where(left, col[:, kind + h : kind + h + 1], col[:, kind + h + 1 : kind + h + 2])
                    parts.append(jnp.where(goal == want, share, 0.0))
            mats.append(jnp.concatenate(parts, axis=0))
        mats = jnp.concatenate(mats, axis=1).astype(BF16)
        for h in range(1, EPG):
            ycopy(p, h).wait_recv()
        for c in range(0, width, 512):
            rows = stack([ybuf[p, h, :, c : c + 512] for h in range(EPG)])
            part = jnp.dot(mats, rows, preferred_element_type=F32)
            for half in range(2):
                both = part[half * group : (half + 1) * group] + part[(2 + half) * group : (3 + half) * group]
                s = 2 * p + half
                into = cbuf if s == HERE else cs
                into[s, :, c : c + 512] = both.astype(BF16)
        for half in range(2):
            if 2 * p + half != HERE:
                ccopy(2 * p + half).start()

    spread(0)
    for copy in loads[2:]:
        copy.wait()
    expert(0)
    spread(1)
    collect(0)
    expert(1)
    spread(2)
    spread(3)
    collect(1)
    expert(2)
    expert(3)
    collect(2)
    collect(3)

    lanes = lax.broadcasted_iota(jnp.int32, (tok, 128), 1)
    back = []
    for p in range(PAIRS):
        there = jnp.where(lanes < 64, lax.rem(z + HOPS[2 * p], planes), lax.rem(z + HOPS[2 * p + 1], planes))
        hit = (cols[:, 0:1] == there.astype(F32)) & (cols[:, 1:2] == (lanes & 63).astype(F32))
        back.append(jnp.where(hit, 1.0, 0.0))
    back = jnp.concatenate(back, axis=1).astype(BF16)
    for s in AWAY:
        ccopy(s).wait_recv()
    for c in range(0, width, 512):
        rows = stack([cbuf[s, :, c : c + 512] for s in range(planes)])
        part = jnp.dot(back, rows, preferred_element_type=F32)
        out_ref[:, c : c + 512] = (hidden[:, c : c + 512] + part).astype(BF16)

    for s in AWAY:
        mcopy(s).wait_send()
        zcopy(s).wait_send()
        ccopy(s).wait_send()
    for p in range(PAIRS):
        for h in range(1, EPG):
            xcopy(p, h).wait_send()
            ycopy(p, h).wait_send()


def layer_kernel(n_sp, n_tp, capacity, parts, *refs):
    cuts = [sum(parts[:i]) for i in range(len(parts) + 1)]
    mixed_in, later_in, out, joined, mixer_scratch, later_scratch = (
        refs[a:b] for a, b in zip(cuts, cuts[1:])
    )
    later = route_and_run(capacity, *joined, *later_in, *out, *later_scratch)
    drain = mix_heads(n_sp, n_tp, lambda: next(later), *mixed_in, *joined, *mixer_scratch)
    for _ in later:
        pass
    drain()


def layer(
    query_rows, key_rows, value_rows, forget_cum, doc_ids, residual, out_weight, norm_gain, expert_ids,
    route_weights, gate, up, down,
):
    n_sp, n_tp = lax.axis_size("sp"), lax.axis_size("tp")
    span, heads = query_rows.shape
    tok, width = residual.shape
    planes = n_sp // EPG
    capacity = max(2, 5 * tok // (4 * planes))
    group = 2 * capacity
    vmem = pl.BlockSpec(memory_space=pltpu.VMEM)
    hbm = pl.BlockSpec(memory_space=pl.ANY)
    dma = pltpu.SemaphoreType.DMA
    slots = pltpu.VMEM((planes, group, width), BF16)
    quads = pltpu.VMEM((PAIRS, EPG, group, width), BF16)
    mixer_scratch = [
        pltpu.VMEM((span, heads), BF16),
        pltpu.VMEM((span, heads), BF16),
        pltpu.VMEM((span, heads), BF16),
        pltpu.VMEM((8, span), F32),
        pltpu.VMEM((span, heads), BF16),
        pltpu.VMEM((span, heads), BF16),
        pltpu.VMEM((8, span), F32),
        pltpu.VMEM((REACH, span, heads), BF16),
        pltpu.VMEM((REACH, span, heads), BF16),
        pltpu.VMEM((REACH, 8, span), F32),
        pltpu.VMEM((2, span, 2 * heads), BF16),
        pltpu.VMEM((2 * heads, span), BF16),
        pltpu.VMEM((2, span, heads), BF16),
        pltpu.VMEM((2, span, 128), F32),
        pltpu.VMEM((2, span, 128), F32),
        pltpu.VMEM((span, heads), BF16),
        pltpu.VMEM((n_tp, tok, heads), BF16),
        dma((3,)),
        dma((1 + 2 * CUTS,)), dma((1 + 2 * CUTS,)),
        dma((REACH, 1 + 2 * CUTS)), dma((REACH, 1 + 2 * CUTS)),
        dma((n_tp,)), dma((n_tp,)),
    ]
    later_scratch = [
        pltpu.VMEM((tok, width), BF16),
        pltpu.VMEM(out_weight.shape, BF16),
        pltpu.VMEM(gate.shape, BF16),
        pltpu.VMEM(up.shape, BF16),
        pltpu.VMEM(down.shape, BF16),
        pltpu.VMEM((tok, width), F32),
        pltpu.VMEM((tok, width), BF16),
        slots, slots,
        pltpu.VMEM((planes, 16, 128), F32),
        pltpu.VMEM((planes, 16, 128), F32),
        pltpu.VMEM((planes, group, 128), F32),
        quads, quads, quads, quads,
        slots, slots,
        dma((5,)),
        dma((planes,)), dma((planes,)), dma((planes,)), dma((planes,)),
        dma((PAIRS, EPG)), dma((PAIRS, EPG)), dma((PAIRS, EPG)), dma((PAIRS, EPG)),
        dma((planes,)), dma((planes,)),
    ]
    parts = (5, 8, 1, 1, len(mixer_scratch), len(later_scratch))
    return pl.pallas_call(
        functools.partial(layer_kernel, n_sp, n_tp, capacity, parts),
        out_shape=jax.ShapeDtypeStruct((tok, width), BF16),
        in_specs=[hbm] * 3 + [vmem] * 5 + [hbm] * 5,
        out_specs=vmem,
        scratch_shapes=[pltpu.VMEM((tok, heads * n_tp), BF16)] + mixer_scratch + later_scratch,
        compiler_params=pltpu.CompilerParams(
            collective_id=0, has_side_effects=True, vmem_limit_bytes=67043328
        ),
        name="layer",
    )(
        query_rows, key_rows, value_rows, forget_cum, doc_ids[None, :], norm_gain[None, :], expert_ids.T,
        route_weights.T, residual, out_weight, gate, up, down,
    )


def per_device(
    query_rows,
    key_rows,
    value_rows,
    forget_cum,
    doc_ids,
    residual,
    out_weight,
    norm_gain,
    expert_ids,
    route_weights,
    gate_proj,
    up_proj,
    down_proj,
):
    return layer(
        query_rows, key_rows, value_rows, forget_cum, doc_ids, residual, out_weight, norm_gain, expert_ids,
        route_weights, gate_proj[0], up_proj[0], down_proj[0],
    )


def solution(mesh):
    placed = (
        P("sp", "tp"),
        P("sp", "tp"),
        P("sp", "tp"),
        P("tp", "sp"),
        P("sp"),
        P(("sp", "tp"), None),
        P(),
        P(),
        P(("sp", "tp"), None),
        P(("sp", "tp"), None),
        P("sp", None, None),
        P("sp", None, None),
        P("sp", None, None),
    )
    return jax.shard_map(
        per_device, mesh=mesh, in_specs=placed, out_specs=P(("sp", "tp"), None), check_vma=False
    )
```

```python
import functools
import jax
import jax.numpy as jnp
from jax import lax
from jax.experimental import pallas as pl
from jax.experimental.pallas import tpu as pltpu
from jax.sharding import PartitionSpec as P

EPG = 4
TOPK = 2
REACH = 3
QT = 512
QF = 1024
KT = 512
FAR = -1e30
CUTS = 2

norm_eps = 1e-06
F32 = jnp.float32
BF16 = jnp.bfloat16


def columns_of(rows):
    parts = [jnp.transpose(rows[:, c : c + 128]) for c in range(0, rows.shape[1], 128)]
    return jnp.concatenate(parts, axis=0).astype(BF16)


def mix_heads(
    n_sp, n_tp, early, q_hbm, k_hbm, v_hbm, gate_ref, doc_ref, out_ref,
    q_ref, k_ref, v_ref, marks_ref, krel, vrel, mrel,
    kbuf, vbuf, mbuf, qaug, keyt, vaug, top, acc, att, heads,
    load, fsend, rsend, rrecv, hsend, hrecv, asend, arecv,
):
    sp = lax.axis_index("sp")
    tp = lax.axis_index("tp")
    tok = q_ref.shape[0]
    chunk = tok // n_tp

    x = lax.rem(sp, EPG)
    z = sp // EPG
    planes = n_sp // EPG

    def along_x(hop):
        return {"sp": z * EPG + lax.rem(x + hop, EPG)}

    def along_z(hop):
        return {"sp": lax.rem(z + hop, planes) * EPG + x}

    barrier = pltpu.get_barrier_semaphore()
    for hop in range(1, EPG):
        pl.semaphore_signal(barrier, inc=1, device_id=along_x(hop))
    for hop in range(1, planes):
        pl.semaphore_signal(barrier, inc=1, device_id=along_z(hop))
    for d in range(1, n_tp):
        pl.semaphore_signal(barrier, inc=1, device_id={"tp": lax.rem(tp + d, n_tp)})

    loads = [
        pltpu.make_async_copy(src, dst, load.at[i])
        for i, (src, dst) in enumerate(((k_hbm, k_ref), (v_hbm, v_ref), (q_hbm, q_ref)))
    ]
    for copy in loads:
        copy.start()
    marks_ref[...] = jnp.concatenate(
        [gate_ref[...], doc_ref[...].astype(F32), jnp.zeros((5, tok), F32)], axis=0
    )
    pl.semaphore_wait(barrier, EPG + planes - 2 + n_tp - 1)

    part = tok // CUTS
    pieces = [(marks_ref, mrel, mbuf, None)]
    for src, rel, buf in ((k_ref, krel, kbuf), (v_ref, vrel, vbuf)):
        pieces += [(src, rel, buf, pl.ds(c * part, part)) for c in range(CUTS)]

    def across(i):
        src, rel, buf, rows = pieces[i]
        if rows is not None:
            src, rel = src.at[rows], rel.at[rows]
        return pltpu.make_async_remote_copy(
            src_ref=src, dst_ref=rel, send_sem=rsend.at[i], recv_sem=rrecv.at[i], device_id=along_z(1)
        )

    def along(i, d, relayed):
        src, rel, buf, rows = pieces[i]
        src = rel if relayed else src
        dst = buf.at[d - 1]
        if rows is not None:
            src, dst = src.at[rows], dst.at[rows]
        return pltpu.make_async_remote_copy(
            src_ref=src, dst_ref=dst, send_sem=hsend.at[d - 1, i], recv_sem=hrecv.at[d - 1, i],
            device_id=along_x(d),
        )

    for i in range(len(pieces)):
        if i in (1, 1 + CUTS):
            loads[0 if i == 1 else 1].wait()

        @pl.when(x > 0)
        def _(i=i):
            across(i).start()

        for d in range(1, REACH + 1):

            @pl.when(x + d < EPG)
            def _(i=i, d=d):
                along(i, d, False).start()

    loads[2].wait()

    def pass_on(i):
        @pl.when(x > 0)
        def _():
            across(i).wait_recv()

        for d in (1, 3):

            @pl.when(x + d >= EPG)
            def _(d=d):
                along(i, d, True).start()

    handing = (x == 1) | (x == 2)

    def hand_on(i):
        buf, rows = pieces[i][2:]
        src, dst = buf.at[2], buf.at[1]
        if rows is not None:
            src, dst = src.at[rows], dst.at[rows]
        return pltpu.make_async_remote_copy(
            src_ref=src, dst_ref=dst, send_sem=fsend.at[i], recv_sem=hrecv.at[1, i], device_id=along_x(3)
        )

    lane = lax.broadcasted_iota(jnp.int32, (1, 128), 1)
    row8 = lax.broadcasted_iota(jnp.int32, (8, tok), 0)
    row16 = lax.broadcasted_iota(jnp.int32, (16, tok), 0).astype(F32)
    blank = jnp.zeros((104, tok), F32)
    own = marks_ref[...]
    base = own[0:2, 0:1]

    same = (own[2:3, :] == row16).astype(F32)
    qmark = columns_of(jnp.concatenate([jnp.zeros((8, tok), F32), same, blank], axis=0))
    qrows = q_ref[...] * jnp.asarray(0.125, BF16)
    for h in range(2):
        mine = (lane >= 64 * h) & (lane < 64 * h + 64)
        ones = (lane >= 3 * h) & (lane < 3 * h + 3)
        qaug[h, :, 0:128] = jnp.where(mine, qrows, jnp.zeros_like(qrows))
        qaug[h, :, 128:256] = jnp.where(ones, jnp.ones_like(qmark), qmark)

    def prepare(marks, keys, v):
        gate = base - marks[0:2, :]
        high = gate.astype(BF16).astype(F32)
        rest = gate - high
        mid = rest.astype(BF16).astype(F32)
        low = rest - mid
        pieces = jnp.zeros((8, tok), F32)
        for h in range(2):
            for i, piece in enumerate((high, mid, low)):
                pieces = jnp.where(row8 == 3 * h + i, piece[h : h + 1, :], pieces)
        other = jnp.where(marks[2:3, :] == row16, 0.0, FAR).astype(F32)
        keyt[128:256, :] = jnp.concatenate([pieces, other, blank], axis=0).astype(BF16)
        for c in range(0, tok, 128):
            keyt[0:128, c : c + 128] = jnp.transpose(keys[c : c + 128, :].astype(F32)).astype(BF16)
        one = jnp.ones_like(v)
        vaug[0] = jnp.where(lane < 64, v, one)
        vaug[1] = jnp.where(lane < 64, one, v)

    def tile(q0, k0, fresh, causal, wide=QT):
        rows = pl.ds(q0, wide)
        for h in range(2):
            score = jnp.dot(qaug[h, rows, :], keyt[:, pl.ds(k0, KT)], preferred_element_type=F32)
            if causal:
                qpos = q0 + lax.broadcasted_iota(jnp.int32, (wide, KT), 0)
                kpos = k0 + lax.broadcasted_iota(jnp.int32, (wide, KT), 1)
                score = jnp.where(kpos <= qpos, score, FAR)
            best = jnp.broadcast_to(jnp.max(score, axis=1, keepdims=True), (wide, 128))
            if not fresh:
                old = top[h, rows, :]
                best = jnp.maximum(best, old)
            expo = jnp.exp(score - jnp.concatenate([best] * (KT // 128), axis=1)).astype(BF16)
            part = jnp.dot(expo, vaug[h, pl.ds(k0, KT), :], preferred_element_type=F32)
            if not fresh:
                part = acc[h, rows, :] * jnp.exp(old - best) + part
            top[h, rows, :] = best
            acc[h, rows, :] = part

    prepare(own, k_ref, v_ref[...])
    tiles = tok // QT
    per = KT // QT
    for k0 in range(0, tok, KT):
        first = k0 // QT

        def diagonal(i, carry, k0=k0):
            tile(pl.multiple_of(i * QT, QT), k0, k0 == 0, True)
            return carry

        def below(i, carry, k0=k0):
            tile(pl.multiple_of(i * QT, QT), k0, k0 == 0, False)
            return carry

        lax.fori_loop(first, first + per, diagonal, 0)
        if first + per < tiles:
            lax.fori_loop(first + per, tiles, below, 0)

    early()
    for i in range(len(pieces)):
        pass_on(i)
    for i in range(len(pieces)):

        @pl.when(handing)
        def _(i=i):
            along(i, 3, False).wait_recv()
            hand_on(i).start()

    for d in range(1, REACH + 1):
        for i in range(len(pieces)):
            if d == 3:

                @pl.when(jnp.logical_not(handing))
                def _(i=i):
                    along(i, 3, False).wait_recv()

            else:
                along(i, d, False).wait_recv()
        prepare(mbuf[d - 1], kbuf.at[d - 1], vbuf[d - 1])
        if d < REACH:

            def full(i, carry):
                for k0 in range(0, tok, KT):
                    tile(pl.multiple_of(i * QF, QF), k0, False, False, QF)
                return carry

            lax.fori_loop(0, tok // QF, full, 0)

    for i in range(tiles):
        q0 = i * QT
        for k0 in range(q0 // KT * KT, tok, KT):
            tile(q0, k0, False, False)
        rows = pl.ds(q0, QT)
        total = jnp.where(lane < 64, pltpu.roll(acc[0, rows, :], 64, 1), pltpu.roll(acc[1, rows, :], 64, 1))
        value = jnp.where(lane < 64, acc[0, rows, :], acc[1, rows, :])
        att[rows, :] = (value / total).astype(BF16)
        for c in range(q0 // chunk, (q0 + QT) // chunk):

            @pl.when(tp != c)
            def _(c=c):
                pltpu.make_async_remote_copy(
                    src_ref=att.at[pl.ds(c * chunk, chunk)], dst_ref=heads.at[tp],
                    send_sem=asend.at[c], recv_sem=arecv.at[tp], device_id={"tp": c},
                ).start()

    for c in range(n_tp):

        @pl.when(tp != c)
        def _(c=c):
            pltpu.make_async_remote_copy(
                src_ref=att.at[pl.ds(c * chunk, chunk)], dst_ref=heads.at[c],
                send_sem=asend.at[c], recv_sem=arecv.at[c], device_id={"tp": c},
            ).wait_recv()
            out_ref[:, c * 128 : (c + 1) * 128] = heads[c]

        @pl.when(tp == c)
        def _(c=c):
            out_ref[:, c * 128 : (c + 1) * 128] = att[c * chunk : (c + 1) * chunk, :]

    def drain():
        for c in range(n_tp):

            @pl.when(tp != c)
            def _(c=c):
                pltpu.make_async_remote_copy(
                    src_ref=att.at[pl.ds(c * chunk, chunk)], dst_ref=heads.at[c],
                    send_sem=asend.at[c], recv_sem=arecv.at[c], device_id={"tp": c},
                ).wait_send()

        for i in range(len(pieces)):

            @pl.when(x > 0)
            def _(i=i):
                across(i).wait_send()

            along(i, 1, False).wait_send()
            along(i, 3, False).wait_send()

            @pl.when(x + 2 < EPG)
            def _(i=i):
                along(i, 2, False).wait_send()

            @pl.when(handing)
            def _(i=i):
                hand_on(i).wait_send()

    return drain


HOPS = (2, 6, 3, 5, 4, 0, 1, 7)
PAIRS = len(HOPS) // 2
HERE = HOPS.index(0)
AWAY = [s for s in range(len(HOPS)) if s != HERE]


def stack(blocks):
    parts = []
    for block in blocks:
        parts += [block.astype(F32), jnp.zeros((64 - block.shape[0], block.shape[1]), F32)]
    return jnp.concatenate(parts, axis=0).astype(BF16)


def route_and_run(
    capacity, heads_ref, gain_ref, ids_ref, weights_ref, residual_hbm, mix_hbm, gate_hbm, up_hbm, down_hbm, out_ref,
    residual_ref, mix, wgate, wup, wdown, hidden, normed, zs, zbuf, ms, mbuf, mcol, xs, xbuf, ys, ybuf, cs, cbuf,
    load, zsend, zrecv, msend, mrecv, xsend, xrecv, ysend, yrecv, csend, crecv,
):
    sp = lax.axis_index("sp")
    x = lax.rem(sp, EPG)
    z = sp // EPG
    planes = len(HOPS)
    group = 2 * capacity
    tok, width = residual_ref.shape
    ffe = wgate.shape[1]

    def along_z(hop):
        return {"sp": lax.rem(z + hop, planes) * EPG + x}

    def along_x(hop):
        return {"sp": z * EPG + lax.rem(x + hop, EPG)}

    loads = [
        pltpu.make_async_copy(src, dst, load.at[i])
        for i, (src, dst) in enumerate(
            ((residual_hbm, residual_ref), (mix_hbm, mix), (gate_hbm, wgate), (up_hbm, wup), (down_hbm, wdown))
        )
    ]
    for copy in loads:
        copy.start()

    ids = ids_ref[...]
    id0, id1 = ids[0:1, :], ids[1:2, :]
    earlier = (
        lax.broadcasted_iota(jnp.int32, (tok, tok), 0) < lax.broadcasted_iota(jnp.int32, (tok, tok), 1)
    ).astype(BF16)
    number = lax.broadcasted_iota(jnp.int32, (planes * EPG, tok), 0)
    uses = ((number == id0) | (number == id1)).astype(F32)
    rank = jnp.dot(uses.astype(BF16), earlier, preferred_element_type=F32)
    row = lax.broadcasted_iota(jnp.int32, (16, tok), 0)
    which = lax.rem(x + row, EPG)
    pick = (
        (lax.broadcasted_iota(jnp.int32, (16, planes * EPG), 1) & (EPG - 1))
        == lax.rem(x + lax.broadcasted_iota(jnp.int32, (16, planes * EPG), 0), EPG)
    ).astype(BF16)
    slots = jnp.dot(pick, (uses * (rank + 1.0)).astype(BF16), preferred_element_type=F32)
    weight = jnp.where((id0 & (EPG - 1)) == which, weights_ref[0:1, :], 0.0) + jnp.where(
        (id1 & (EPG - 1)) == which, weights_ref[1:2, :], 0.0
    )
    high = weight.astype(BF16).astype(F32)
    info = jnp.where(row < 4, slots, jnp.where(row < 8, high, jnp.where(row < 12, weight - high, 0.0)))
    info = info.astype(BF16)
    mine = lax.shift_right_logical(id0, 2)
    member = (lax.broadcasted_iota(jnp.int32, (planes, tok), 0) == mine).astype(F32)
    place = jnp.sum(
        member * jnp.dot(member.astype(BF16), earlier, preferred_element_type=F32), axis=0, keepdims=True
    )
    mine = mine.astype(F32)
    spot = lax.broadcasted_iota(jnp.int32, (group, tok), 0).astype(F32)
    sel = []
    for hop in HOPS:
        there = lax.rem(z + hop, planes).astype(F32)
        sel.append(jnp.where((mine == there) & (place == spot), 1.0, 0.0))
    for s in range(planes):
        table = lax.dot_general(
            info, sel[s].astype(BF16), (((1,), (1,)), ((), ())), preferred_element_type=F32
        )
        rest = jnp.zeros((16, 64 - group), F32)
        table = [table, rest, jnp.zeros((16, 64), F32)] if s % 2 == 0 else [jnp.zeros((16, 64), F32), table, rest]
        table = jnp.concatenate(table, axis=1)
        if s == HERE:
            mbuf[s] = table
        else:
            ms[s] = table
    sel = jnp.concatenate(sel, axis=0).astype(BF16)
    wide = lax.broadcasted_iota(jnp.int32, (tok, tok), 0)
    cols = jnp.transpose(jnp.where(wide == 0, mine, jnp.where(wide == 1, place, 0.0)))

    yield

    loads[0].wait()
    loads[1].wait()
    square = jnp.zeros((tok, 128), F32)
    for c in range(0, width, 512):
        part = jnp.dot(heads_ref[...], mix[:, c : c + 512], preferred_element_type=F32)
        part = part + residual_ref[:, c : c + 512].astype(F32)
        hidden[:, c : c + 512] = part
        for i in range(0, 512, 128):
            square = square + part[:, i : i + 128] * part[:, i : i + 128]
    scale = lax.rsqrt(jnp.sum(square, axis=1, keepdims=True) / width + norm_eps)
    for c in range(0, width, 512):
        normed[:, c : c + 512] = (
            hidden[:, c : c + 512] * scale * gain_ref[:, c : c + 512]
        ).astype(BF16)

    for c in range(0, width, 512):
        part = jnp.dot(sel, normed[:, c : c + 512], preferred_element_type=F32)
        for s in range(planes):
            into = zbuf if s == HERE else zs
            into[s, :, c : c + 512] = part[s * group : (s + 1) * group].astype(BF16)

    def zcopy(s):
        return pltpu.make_async_remote_copy(
            src_ref=zs.at[s], dst_ref=zbuf.at[s], send_sem=zsend.at[s], recv_sem=zrecv.at[s],
            device_id=along_z(HOPS[s]),
        )

    def mcopy(s):
        return pltpu.make_async_remote_copy(
            src_ref=ms.at[s], dst_ref=mbuf.at[s], send_sem=msend.at[s], recv_sem=mrecv.at[s],
            device_id=along_z(HOPS[s]),
        )

    def xcopy(p, hop):
        return pltpu.make_async_remote_copy(
            src_ref=xs.at[p, hop], dst_ref=xbuf.at[p, hop], send_sem=xsend.at[p, hop],
            recv_sem=xrecv.at[p, hop], device_id=along_x(hop),
        )

    def ycopy(p, hop):
        return pltpu.make_async_remote_copy(
            src_ref=ys.at[p, hop], dst_ref=ybuf.at[p, hop], send_sem=ysend.at[p, hop],
            recv_sem=yrecv.at[p, hop], device_id=along_x(EPG - hop),
        )

    def ccopy(s):
        return pltpu.make_async_remote_copy(
            src_ref=cs.at[s], dst_ref=cbuf.at[s], send_sem=csend.at[s], recv_sem=crecv.at[s],
            device_id=along_z(planes - HOPS[s]),
        )

    for s in AWAY:
        mcopy(s).start()
        zcopy(s).start()

    def spread(p):
        for half in range(2):
            s = 2 * p + half
            if s != HERE:
                mcopy(s).wait_recv()
            table = jnp.concatenate([mbuf[s], jnp.zeros((112, 128), F32)], axis=0)
            mcol[s] = jnp.transpose(table)[64 * half : 64 * half + group, :]
        second = mbuf[2 * p + 1]
        table = mbuf[2 * p] + jnp.where(second > 0.0, second + float(capacity), 0.0)
        want = lax.broadcasted_iota(jnp.int32, (group, 128), 0).astype(F32) + 1.0
        rows = [jnp.where(table[h : h + 1, :] == want, 1.0, 0.0) for h in range(EPG)]
        order = jnp.concatenate(rows, axis=0).astype(BF16)
        for half in range(2):
            if 2 * p + half != HERE:
                zcopy(2 * p + half).wait_recv()
        for c in range(0, width, 512):
            rows = stack([zbuf[2 * p, :, c : c + 512], zbuf[2 * p + 1, :, c : c + 512]])
            part = jnp.dot(order, rows, preferred_element_type=F32)
            xbuf[p, 0, :, c : c + 512] = part[0:group].astype(BF16)
            for h in range(1, EPG):
                xs[p, h, :, c : c + 512] = part[h * group : (h + 1) * group].astype(BF16)
        for h in range(1, EPG):
            xcopy(p, h).start()

    def expert(p):
        for h in range(1, EPG):
            xcopy(p, h).wait_recv()
        gate = jnp.zeros((EPG * group, ffe), F32)
        up = jnp.zeros((EPG * group, ffe), F32)
        for c in range(0, width, 512):
            rows = jnp.concatenate(
                [xbuf[p, h, :, c : c + 512].astype(F32) for h in range(EPG)], axis=0
            ).astype(BF16)
            gate = gate + jnp.dot(rows, wgate[c : c + 512, :], preferred_element_type=F32)
            up = up + jnp.dot(rows, wup[c : c + 512, :], preferred_element_type=F32)
        act = (gate / (1.0 + jnp.exp(-gate)) * up).astype(BF16)
        for c in range(0, width, 512):
            part = jnp.dot(act, wdown[:, c : c + 512], preferred_element_type=F32)
            ybuf[p, 0, :, c : c + 512] = part[0:group].astype(BF16)
            for h in range(1, EPG):
                ys[p, h, :, c : c + 512] = part[h * group : (h + 1) * group].astype(BF16)
        for h in range(1, EPG):
            ycopy(p, h).start()

    def collect(p):
        lanes = lax.broadcasted_iota(jnp.int32, (group, 128), 1)
        left = lanes < 64
        want = ((lanes & 63) + 1).astype(F32)
        mats = []
        for h in range(0, EPG, 2):
            parts = []
            for kind in (4, 8):
                for half in range(2):
                    col = mcol[2 * p + half]
                    goal = jnp.where(left, col[:, h : h + 1], col[:, h + 1 : h + 2])
                    goal = jnp.where(goal > 0.0, goal + float(half * capacity), 0.0)
                    share = jnp.where(left, col[:, kind + h : kind + h + 1], col[:, kind + h + 1 : kind + h + 2])
                    parts.append(jnp.where(goal == want, share, 0.0))
            mats.append(jnp.concatenate(parts, axis=0))
        mats = jnp.concatenate(mats, axis=1).astype(BF16)
        for h in range(1, EPG):
            ycopy(p, h).wait_recv()
        for c in range(0, width, 512):
            rows = stack([ybuf[p, h, :, c : c + 512] for h in range(EPG)])
            part = jnp.dot(mats, rows, preferred_element_type=F32)
            for half in range(2):
                both = part[half * group : (half + 1) * group] + part[(2 + half) * group : (3 + half) * group]
                s = 2 * p + half
                into = cbuf if s == HERE else cs
                into[s, :, c : c + 512] = both.astype(BF16)
        for half in range(2):
            if 2 * p + half != HERE:
                ccopy(2 * p + half).start()

    spread(0)
    for copy in loads[2:]:
        copy.wait()
    expert(0)
    spread(1)
    collect(0)
    expert(1)
    spread(2)
    spread(3)
    collect(1)
    expert(2)
    expert(3)
    collect(2)
    collect(3)

    lanes = lax.broadcasted_iota(jnp.int32, (tok, 128), 1)
    back = []
    for p in range(PAIRS):
        there = jnp.where(lanes < 64, lax.rem(z + HOPS[2 * p], planes), lax.rem(z + HOPS[2 * p + 1], planes))
        hit = (cols[:, 0:1] == there.astype(F32)) & (cols[:, 1:2] == (lanes & 63).astype(F32))
        back.append(jnp.where(hit, 1.0, 0.0))
    back = jnp.concatenate(back, axis=1).astype(BF16)
    for s in AWAY:
        ccopy(s).wait_recv()
    for c in range(0, width, 512):
        rows = stack([cbuf[s, :, c : c + 512] for s in range(planes)])
        part = jnp.dot(back, rows, preferred_element_type=F32)
        out_ref[:, c : c + 512] = (hidden[:, c : c + 512] + part).astype(BF16)

    for s in AWAY:
        mcopy(s).wait_send()
        zcopy(s).wait_send()
        ccopy(s).wait_send()
    for p in range(PAIRS):
        for h in range(1, EPG):
            xcopy(p, h).wait_send()
            ycopy(p, h).wait_send()


def layer_kernel(n_sp, n_tp, capacity, parts, *refs):
    cuts = [sum(parts[:i]) for i in range(len(parts) + 1)]
    mixed_in, later_in, out, joined, mixer_scratch, later_scratch = (
        refs[a:b] for a, b in zip(cuts, cuts[1:])
    )
    later = route_and_run(capacity, *joined, *later_in, *out, *later_scratch)
    drain = mix_heads(n_sp, n_tp, lambda: next(later), *mixed_in, *joined, *mixer_scratch)
    for _ in later:
        pass
    drain()


def layer(
    query_rows, key_rows, value_rows, forget_cum, doc_ids, residual, out_weight, norm_gain, expert_ids,
    route_weights, gate, up, down,
):
    n_sp, n_tp = lax.axis_size("sp"), lax.axis_size("tp")
    span, heads = query_rows.shape
    tok, width = residual.shape
    planes = n_sp // EPG
    capacity = max(2, 5 * tok // (4 * planes))
    group = 2 * capacity
    vmem = pl.BlockSpec(memory_space=pltpu.VMEM)
    hbm = pl.BlockSpec(memory_space=pl.ANY)
    dma = pltpu.SemaphoreType.DMA
    slots = pltpu.VMEM((planes, group, width), BF16)
    quads = pltpu.VMEM((PAIRS, EPG, group, width), BF16)
    mixer_scratch = [
        pltpu.VMEM((span, heads), BF16),
        pltpu.VMEM((span, heads), BF16),
        pltpu.VMEM((span, heads), BF16),
        pltpu.VMEM((8, span), F32),
        pltpu.VMEM((span, heads), BF16),
        pltpu.VMEM((span, heads), BF16),
        pltpu.VMEM((8, span), F32),
        pltpu.VMEM((REACH, span, heads), BF16),
        pltpu.VMEM((REACH, span, heads), BF16),
        pltpu.VMEM((REACH, 8, span), F32),
        pltpu.VMEM((2, span, 2 * heads), BF16),
        pltpu.VMEM((2 * heads, span), BF16),
        pltpu.VMEM((2, span, heads), BF16),
        pltpu.VMEM((2, span, 128), F32),
        pltpu.VMEM((2, span, 128), F32),
        pltpu.VMEM((span, heads), BF16),
        pltpu.VMEM((n_tp, tok, heads), BF16),
        dma((3,)),
        dma((1 + 2 * CUTS,)), dma((1 + 2 * CUTS,)), dma((1 + 2 * CUTS,)),
        dma((REACH, 1 + 2 * CUTS)), dma((REACH, 1 + 2 * CUTS)),
        dma((n_tp,)), dma((n_tp,)),
    ]
    later_scratch = [
        pltpu.VMEM((tok, width), BF16),
        pltpu.VMEM(out_weight.shape, BF16),
        pltpu.VMEM(gate.shape, BF16),
        pltpu.VMEM(up.shape, BF16),
        pltpu.VMEM(down.shape, BF16),
        pltpu.VMEM((tok, width), F32),
        pltpu.VMEM((tok, width), BF16),
        slots, slots,
        pltpu.VMEM((planes, 16, 128), F32),
        pltpu.VMEM((planes, 16, 128), F32),
        pltpu.VMEM((planes, group, 128), F32),
        quads, quads, quads, quads,
        slots, slots,
        dma((5,)),
        dma((planes,)), dma((planes,)), dma((planes,)), dma((planes,)),
        dma((PAIRS, EPG)), dma((PAIRS, EPG)), dma((PAIRS, EPG)), dma((PAIRS, EPG)),
        dma((planes,)), dma((planes,)),
    ]
    parts = (5, 8, 1, 1, len(mixer_scratch), len(later_scratch))
    return pl.pallas_call(
        functools.partial(layer_kernel, n_sp, n_tp, capacity, parts),
        out_shape=jax.ShapeDtypeStruct((tok, width), BF16),
        in_specs=[hbm] * 3 + [vmem] * 5 + [hbm] * 5,
        out_specs=vmem,
        scratch_shapes=[pltpu.VMEM((tok, heads * n_tp), BF16)] + mixer_scratch + later_scratch,
        compiler_params=pltpu.CompilerParams(
            collective_id=0, has_side_effects=True, vmem_limit_bytes=67043328
        ),
        name="layer",
    )(
        query_rows, key_rows, value_rows, forget_cum, doc_ids[None, :], norm_gain[None, :], expert_ids.T,
        route_weights.T, residual, out_weight, gate, up, down,
    )


def per_device(
    query_rows,
    key_rows,
    value_rows,
    forget_cum,
    doc_ids,
    residual,
    out_weight,
    norm_gain,
    expert_ids,
    route_weights,
    gate_proj,
    up_proj,
    down_proj,
):
    return layer(
        query_rows, key_rows, value_rows, forget_cum, doc_ids, residual, out_weight, norm_gain, expert_ids,
        route_weights, gate_proj[0], up_proj[0], down_proj[0],
    )


def solution(mesh):
    placed = (
        P("sp", "tp"),
        P("sp", "tp"),
        P("sp", "tp"),
        P("tp", "sp"),
        P("sp"),
        P(("sp", "tp"), None),
        P(),
        P(),
        P(("sp", "tp"), None),
        P(("sp", "tp"), None),
        P("sp", None, None),
        P("sp", None, None),
        P("sp", None, None),
    )
    return jax.shard_map(
        per_device, mesh=mesh, in_specs=placed, out_specs=P(("sp", "tp"), None), check_vma=False
    )
```

```python
import functools
import jax
import jax.numpy as jnp
from jax import lax
from jax.experimental import pallas as pl
from jax.experimental.pallas import tpu as pltpu
from jax.sharding import PartitionSpec as P

EPG = 4
TOPK = 2
REACH = 3
QT = 512
QF = 1024
KT = 512
FAR = -1e30
CUTS = 4

norm_eps = 1e-06
F32 = jnp.float32
BF16 = jnp.bfloat16


def columns_of(rows):
    parts = [jnp.transpose(rows[:, c : c + 128]) for c in range(0, rows.shape[1], 128)]
    return jnp.concatenate(parts, axis=0).astype(BF16)


def mix_heads(
    n_sp, n_tp, early, q_hbm, k_hbm, v_hbm, gate_ref, doc_ref, out_ref,
    q_ref, k_ref, v_ref, marks_ref, krel, vrel, mrel,
    kbuf, vbuf, mbuf, qaug, keyt, vaug, top, acc, att, heads,
    load, fsend, rsend, rrecv, hsend, hrecv, asend, arecv,
):
    sp = lax.axis_index("sp")
    tp = lax.axis_index("tp")
    tok = q_ref.shape[0]
    chunk = tok // n_tp

    x = lax.rem(sp, EPG)
    z = sp // EPG
    planes = n_sp // EPG

    def along_x(hop):
        return {"sp": z * EPG + lax.rem(x + hop, EPG)}

    def along_z(hop):
        return {"sp": lax.rem(z + hop, planes) * EPG + x}

    barrier = pltpu.get_barrier_semaphore()
    for hop in range(1, EPG):
        pl.semaphore_signal(barrier, inc=1, device_id=along_x(hop))
    for hop in range(1, planes):
        pl.semaphore_signal(barrier, inc=1, device_id=along_z(hop))
    for d in range(1, n_tp):
        pl.semaphore_signal(barrier, inc=1, device_id={"tp": lax.rem(tp + d, n_tp)})

    loads = [
        pltpu.make_async_copy(src, dst, load.at[i])
        for i, (src, dst) in enumerate(((k_hbm, k_ref), (v_hbm, v_ref), (q_hbm, q_ref)))
    ]
    for copy in loads:
        copy.start()
    marks_ref[...] = jnp.concatenate(
        [gate_ref[...], doc_ref[...].astype(F32), jnp.zeros((5, tok), F32)], axis=0
    )
    pl.semaphore_wait(barrier, EPG + planes - 2 + n_tp - 1)

    part = tok // CUTS
    pieces = [(marks_ref, mrel, mbuf, None)]
    for src, rel, buf in ((k_ref, krel, kbuf), (v_ref, vrel, vbuf)):
        pieces += [(src, rel, buf, pl.ds(c * part, part)) for c in range(CUTS)]

    def across(i):
        src, rel, buf, rows = pieces[i]
        if rows is not None:
            src, rel = src.at[rows], rel.at[rows]
        return pltpu.make_async_remote_copy(
            src_ref=src, dst_ref=rel, send_sem=rsend.at[i], recv_sem=rrecv.at[i], device_id=along_z(1)
        )

    def along(i, d, relayed):
        src, rel, buf, rows = pieces[i]
        src = rel if relayed else src
        dst = buf.at[d - 1]
        if rows is not None:
            src, dst = src.at[rows], dst.at[rows]
        return pltpu.make_async_remote_copy(
            src_ref=src, dst_ref=dst, send_sem=hsend.at[d - 1, i], recv_sem=hrecv.at[d - 1, i],
            device_id=along_x(d),
        )

    for i in range(len(pieces)):
        if i in (1, 1 + CUTS):
            loads[0 if i == 1 else 1].wait()

        @pl.when(x > 0)
        def _(i=i):
            across(i).start()

        for d in range(1, REACH + 1):

            @pl.when(x + d < EPG)
            def _(i=i, d=d):
                along(i, d, False).start()

    loads[2].wait()

    def pass_on(i):
        @pl.when(x > 0)
        def _():
            across(i).wait_recv()

        for d in (1, 3):

            @pl.when(x + d >= EPG)
            def _(d=d):
                along(i, d, True).start()

    handing = (x == 1) | (x == 2)

    def hand_on(i):
        buf, rows = pieces[i][2:]
        src, dst = buf.at[2], buf.at[1]
        if rows is not None:
            src, dst = src.at[rows], dst.at[rows]
        return pltpu.make_async_remote_copy(
            src_ref=src, dst_ref=dst, send_sem=fsend.at[i], recv_sem=hrecv.at[1, i], device_id=along_x(3)
        )

    lane = lax.broadcasted_iota(jnp.int32, (1, 128), 1)
    row8 = lax.broadcasted_iota(jnp.int32, (8, tok), 0)
    row16 = lax.broadcasted_iota(jnp.int32, (16, tok), 0).astype(F32)
    blank = jnp.zeros((104, tok), F32)
    own = marks_ref[...]
    base = own[0:2, 0:1]

    same = (own[2:3, :] == row16).astype(F32)
    qmark = columns_of(jnp.concatenate([jnp.zeros((8, tok), F32), same, blank], axis=0))
    qrows = q_ref[...] * jnp.asarray(0.125, BF16)
    for h in range(2):
        mine = (lane >= 64 * h) & (lane < 64 * h + 64)
        ones = (lane >= 3 * h) & (lane < 3 * h + 3)
        qaug[h, :, 0:128] = jnp.where(mine, qrows, jnp.zeros_like(qrows))
        qaug[h, :, 128:256] = jnp.where(ones, jnp.ones_like(qmark), qmark)

    def prepare(marks, keys, v):
        gate = base - marks[0:2, :]
        high = gate.astype(BF16).astype(F32)
        rest = gate - high
        mid = rest.astype(BF16).astype(F32)
        low = rest - mid
        pieces = jnp.zeros((8, tok), F32)
        for h in range(2):
            for i, piece in enumerate((high, mid, low)):
                pieces = jnp.where(row8 == 3 * h + i, piece[h : h + 1, :], pieces)
        other = jnp.where(marks[2:3, :] == row16, 0.0, FAR).astype(F32)
        keyt[128:256, :] = jnp.concatenate([pieces, other, blank], axis=0).astype(BF16)
        for c in range(0, tok, 128):
            keyt[0:128, c : c + 128] = jnp.transpose(keys[c : c + 128, :].astype(F32)).astype(BF16)
        one = jnp.ones_like(v)
        vaug[0] = jnp.where(lane < 64, v, one)
        vaug[1] = jnp.where(lane < 64, one, v)

    def tile(q0, k0, fresh, causal, wide=QT):
        rows = pl.ds(q0, wide)
        for h in range(2):
            score = jnp.dot(qaug[h, rows, :], keyt[:, pl.ds(k0, KT)], preferred_element_type=F32)
            if causal:
                qpos = q0 + lax.broadcasted_iota(jnp.int32, (wide, KT), 0)
                kpos = k0 + lax.broadcasted_iota(jnp.int32, (wide, KT), 1)
                score = jnp.where(kpos <= qpos, score, FAR)
            best = jnp.broadcast_to(jnp.max(score, axis=1, keepdims=True), (wide, 128))
            if not fresh:
                old = top[h, rows, :]
                best = jnp.maximum(best, old)
            expo = jnp.exp(score - jnp.concatenate([best] * (KT // 128), axis=1)).astype(BF16)
            part = jnp.dot(expo, vaug[h, pl.ds(k0, KT), :], preferred_element_type=F32)
            if not fresh:
                part = acc[h, rows, :] * jnp.exp(old - best) + part
            top[h, rows, :] = best
            acc[h, rows, :] = part

    prepare(own, k_ref, v_ref[...])
    tiles = tok // QT
    per = KT // QT
    for k0 in range(0, tok, KT):
        first = k0 // QT

        def diagonal(i, carry, k0=k0):
            tile(pl.multiple_of(i * QT, QT), k0, k0 == 0, True)
            return carry

        def below(i, carry, k0=k0):
            tile(pl.multiple_of(i * QT, QT), k0, k0 == 0, False)
            return carry

        lax.fori_loop(first, first + per, diagonal, 0)
        if first + per < tiles:
            lax.fori_loop(first + per, tiles, below, 0)

    early()
    for i in range(len(pieces)):
        pass_on(i)
    for i in range(len(pieces)):

        @pl.when(handing)
        def _(i=i):
            along(i, 3, False).wait_recv()
            hand_on(i).start()

    for d in range(1, REACH + 1):
        for i in range(len(pieces)):
            if d == 3:

                @pl.when(jnp.logical_not(handing))
                def _(i=i):
                    along(i, 3, False).wait_recv()

            else:
                along(i, d, False).wait_recv()
        prepare(mbuf[d - 1], kbuf.at[d - 1], vbuf[d - 1])
        if d < REACH:

            def full(i, carry):
                for k0 in range(0, tok, KT):
                    tile(pl.multiple_of(i * QF, QF), k0, False, False, QF)
                return carry

            lax.fori_loop(0, tok // QF, full, 0)

    for i in range(tiles):
        q0 = i * QT
        for k0 in range(q0 // KT * KT, tok, KT):
            tile(q0, k0, False, False)
        rows = pl.ds(q0, QT)
        total = jnp.where(lane < 64, pltpu.roll(acc[0, rows, :], 64, 1), pltpu.roll(acc[1, rows, :], 64, 1))
        value = jnp.where(lane < 64, acc[0, rows, :], acc[1, rows, :])
        att[rows, :] = (value / total).astype(BF16)
        for c in range(q0 // chunk, (q0 + QT) // chunk):

            @pl.when(tp != c)
            def _(c=c):
                pltpu.make_async_remote_copy(
                    src_ref=att.at[pl.ds(c * chunk, chunk)], dst_ref=heads.at[tp],
                    send_sem=asend.at[c], recv_sem=arecv.at[tp], device_id={"tp": c},
                ).start()

    for c in range(n_tp):

        @pl.when(tp != c)
        def _(c=c):
            pltpu.make_async_remote_copy(
                src_ref=att.at[pl.ds(c * chunk, chunk)], dst_ref=heads.at[c],
                send_sem=asend.at[c], recv_sem=arecv.at[c], device_id={"tp": c},
            ).wait_recv()
            out_ref[:, c * 128 : (c + 1) * 128] = heads[c]

        @pl.when(tp == c)
        def _(c=c):
            out_ref[:, c * 128 : (c + 1) * 128] = att[c * chunk : (c + 1) * chunk, :]

    def drain():
        for c in range(n_tp):

            @pl.when(tp != c)
            def _(c=c):
                pltpu.make_async_remote_copy(
                    src_ref=att.at[pl.ds(c * chunk, chunk)], dst_ref=heads.at[c],
                    send_sem=asend.at[c], recv_sem=arecv.at[c], device_id={"tp": c},
                ).wait_send()

        for i in range(len(pieces)):

            @pl.when(x > 0)
            def _(i=i):
                across(i).wait_send()

            along(i, 1, False).wait_send()
            along(i, 3, False).wait_send()

            @pl.when(x + 2 < EPG)
            def _(i=i):
                along(i, 2, False).wait_send()

            @pl.when(handing)
            def _(i=i):
                hand_on(i).wait_send()

    return drain


HOPS = (2, 6, 3, 5, 4, 0, 1, 7)
PAIRS = len(HOPS) // 2
HERE = HOPS.index(0)
AWAY = [s for s in range(len(HOPS)) if s != HERE]


def stack(blocks):
    parts = []
    for block in blocks:
        parts += [block.astype(F32), jnp.zeros((64 - block.shape[0], block.shape[1]), F32)]
    return jnp.concatenate(parts, axis=0).astype(BF16)


def route_and_run(
    capacity, heads_ref, gain_ref, ids_ref, weights_ref, residual_hbm, mix_hbm, gate_hbm, up_hbm, down_hbm, out_ref,
    residual_ref, mix, wgate, wup, wdown, hidden, normed, zs, zbuf, ms, mbuf, mcol, xs, xbuf, ys, ybuf, cs, cbuf,
    load, zsend, zrecv, msend, mrecv, xsend, xrecv, ysend, yrecv, csend, crecv,
):
    sp = lax.axis_index("sp")
    x = lax.rem(sp, EPG)
    z = sp // EPG
    planes = len(HOPS)
    group = 2 * capacity
    tok, width = residual_ref.shape
    ffe = wgate.shape[1]

    def along_z(hop):
        return {"sp": lax.rem(z + hop, planes) * EPG + x}

    def along_x(hop):
        return {"sp": z * EPG + lax.rem(x + hop, EPG)}

    loads = [
        pltpu.make_async_copy(src, dst, load.at[i])
        for i, (src, dst) in enumerate(
            ((residual_hbm, residual_ref), (mix_hbm, mix), (gate_hbm, wgate), (up_hbm, wup), (down_hbm, wdown))
        )
    ]
    for copy in loads:
        copy.start()

    ids = ids_ref[...]
    id0, id1 = ids[0:1, :], ids[1:2, :]
    earlier = (
        lax.broadcasted_iota(jnp.int32, (tok, tok), 0) < lax.broadcasted_iota(jnp.int32, (tok, tok), 1)
    ).astype(BF16)
    number = lax.broadcasted_iota(jnp.int32, (planes * EPG, tok), 0)
    uses = ((number == id0) | (number == id1)).astype(F32)
    rank = jnp.dot(uses.astype(BF16), earlier, preferred_element_type=F32)
    row = lax.broadcasted_iota(jnp.int32, (16, tok), 0)
    which = lax.rem(x + row, EPG)
    pick = (
        (lax.broadcasted_iota(jnp.int32, (16, planes * EPG), 1) & (EPG - 1))
        == lax.rem(x + lax.broadcasted_iota(jnp.int32, (16, planes * EPG), 0), EPG)
    ).astype(BF16)
    slots = jnp.dot(pick, (uses * (rank + 1.0)).astype(BF16), preferred_element_type=F32)
    weight = jnp.where((id0 & (EPG - 1)) == which, weights_ref[0:1, :], 0.0) + jnp.where(
        (id1 & (EPG - 1)) == which, weights_ref[1:2, :], 0.0
    )
    high = weight.astype(BF16).astype(F32)
    info = jnp.where(row < 4, slots, jnp.where(row < 8, high, jnp.where(row < 12, weight - high, 0.0)))
    info = info.astype(BF16)
    mine = lax.shift_right_logical(id0, 2)
    member = (lax.broadcasted_iota(jnp.int32, (planes, tok), 0) == mine).astype(F32)
    place = jnp.sum(
        member * jnp.dot(member.astype(BF16), earlier, preferred_element_type=F32), axis=0, keepdims=True
    )
    mine = mine.astype(F32)
    spot = lax.broadcasted_iota(jnp.int32, (group, tok), 0).astype(F32)
    sel = []
    for hop in HOPS:
        there = lax.rem(z + hop, planes).astype(F32)
        sel.append(jnp.where((mine == there) & (place == spot), 1.0, 0.0))
    for s in range(planes):
        table = lax.dot_general(
            info, sel[s].astype(BF16), (((1,), (1,)), ((), ())), preferred_element_type=F32
        )
        rest = jnp.zeros((16, 64 - group), F32)
        table = [table, rest, jnp.zeros((16, 64), F32)] if s % 2 == 0 else [jnp.zeros((16, 64), F32), table, rest]
        table = jnp.concatenate(table, axis=1)
        if s == HERE:
            mbuf[s] = table.astype(BF16)
        else:
            ms[s] = table.astype(BF16)
    sel = jnp.concatenate(sel, axis=0).astype(BF16)
    wide = lax.broadcasted_iota(jnp.int32, (tok, tok), 0)
    cols = jnp.transpose(jnp.where(wide == 0, mine, jnp.where(wide == 1, place, 0.0)))

    yield

    loads[0].wait()
    loads[1].wait()
    square = jnp.zeros((tok, 128), F32)
    for c in range(0, width, 512):
        part = jnp.dot(heads_ref[...], mix[:, c : c + 512], preferred_element_type=F32)
        part = part + residual_ref[:, c : c + 512].astype(F32)
        hidden[:, c : c + 512] = part
        for i in range(0, 512, 128):
            square = square + part[:, i : i + 128] * part[:, i : i + 128]
    scale = lax.rsqrt(jnp.sum(square, axis=1, keepdims=True) / width + norm_eps)
    for c in range(0, width, 512):
        normed[:, c : c + 512] = (
            hidden[:, c : c + 512] * scale * gain_ref[:, c : c + 512]
        ).astype(BF16)

    for c in range(0, width, 512):
        part = jnp.dot(sel, normed[:, c : c + 512], preferred_element_type=F32)
        for s in range(planes):
            into = zbuf if s == HERE else zs
            into[s, :, c : c + 512] = part[s * group : (s + 1) * group].astype(BF16)

    def zcopy(s):
        return pltpu.make_async_remote_copy(
            src_ref=zs.at[s], dst_ref=zbuf.at[s], send_sem=zsend.at[s], recv_sem=zrecv.at[s],
            device_id=along_z(HOPS[s]),
        )

    def mcopy(s):
        return pltpu.make_async_remote_copy(
            src_ref=ms.at[s], dst_ref=mbuf.at[s], send_sem=msend.at[s], recv_sem=mrecv.at[s],
            device_id=along_z(HOPS[s]),
        )

    def xcopy(p, hop):
        return pltpu.make_async_remote_copy(
            src_ref=xs.at[p, hop], dst_ref=xbuf.at[p, hop], send_sem=xsend.at[p, hop],
            recv_sem=xrecv.at[p, hop], device_id=along_x(hop),
        )

    def ycopy(p, hop):
        return pltpu.make_async_remote_copy(
            src_ref=ys.at[p, hop], dst_ref=ybuf.at[p, hop], send_sem=ysend.at[p, hop],
            recv_sem=yrecv.at[p, hop], device_id=along_x(EPG - hop),
        )

    def ccopy(s):
        return pltpu.make_async_remote_copy(
            src_ref=cs.at[s], dst_ref=cbuf.at[s], send_sem=csend.at[s], recv_sem=crecv.at[s],
            device_id=along_z(planes - HOPS[s]),
        )

    for s in AWAY:
        mcopy(s).start()
        zcopy(s).start()

    def spread(p):
        for half in range(2):
            s = 2 * p + half
            if s != HERE:
                mcopy(s).wait_recv()
            table = jnp.concatenate([mbuf[s].astype(F32), jnp.zeros((112, 128), F32)], axis=0)
            mcol[s] = jnp.transpose(table)[64 * half : 64 * half + group, :]
        second = mbuf[2 * p + 1].astype(F32)
        table = mbuf[2 * p].astype(F32) + jnp.where(second > 0.0, second + float(capacity), 0.0)
        want = lax.broadcasted_iota(jnp.int32, (group, 128), 0).astype(F32) + 1.0
        rows = [jnp.where(table[h : h + 1, :] == want, 1.0, 0.0) for h in range(EPG)]
        order = jnp.concatenate(rows, axis=0).astype(BF16)
        for half in range(2):
            if 2 * p + half != HERE:
                zcopy(2 * p + half).wait_recv()
        for c in range(0, width, 512):
            rows = stack([zbuf[2 * p, :, c : c + 512], zbuf[2 * p + 1, :, c : c + 512]])
            part = jnp.dot(order, rows, preferred_element_type=F32)
            xbuf[p, 0, :, c : c + 512] = part[0:group].astype(BF16)
            for h in range(1, EPG):
                xs[p, h, :, c : c + 512] = part[h * group : (h + 1) * group].astype(BF16)
        for h in range(1, EPG):
            xcopy(p, h).start()

    def expert(p):
        for h in range(1, EPG):
            xcopy(p, h).wait_recv()
        gate = jnp.zeros((EPG * group, ffe), F32)
        up = jnp.zeros((EPG * group, ffe), F32)
        for c in range(0, width, 512):
            rows = jnp.concatenate(
                [xbuf[p, h, :, c : c + 512].astype(F32) for h in range(EPG)], axis=0
            ).astype(BF16)
            gate = gate + jnp.dot(rows, wgate[c : c + 512, :], preferred_element_type=F32)
            up = up + jnp.dot(rows, wup[c : c + 512, :], preferred_element_type=F32)
        act = (gate / (1.0 + jnp.exp(-gate)) * up).astype(BF16)
        for c in range(0, width, 512):
            part = jnp.dot(act, wdown[:, c : c + 512], preferred_element_type=F32)
            ybuf[p, 0, :, c : c + 512] = part[0:group].astype(BF16)
            for h in range(1, EPG):
                ys[p, h, :, c : c + 512] = part[h * group : (h + 1) * group].astype(BF16)
        for h in range(1, EPG):
            ycopy(p, h).start()

    def collect(p):
        lanes = lax.broadcasted_iota(jnp.int32, (group, 128), 1)
        left = lanes < 64
        want = ((lanes & 63) + 1).astype(F32)
        mats = []
        for h in range(0, EPG, 2):
            parts = []
            for kind in (4, 8):
                for half in range(2):
                    col = mcol[2 * p + half]
                    goal = jnp.where(left, col[:, h : h + 1], col[:, h + 1 : h + 2])
                    goal = jnp.where(goal > 0.0, goal + float(half * capacity), 0.0)
                    share = jnp.where(left, col[:, kind + h : kind + h + 1], col[:, kind + h + 1 : kind + h + 2])
                    parts.append(jnp.where(goal == want, share, 0.0))
            mats.append(jnp.concatenate(parts, axis=0))
        mats = jnp.concatenate(mats, axis=1).astype(BF16)
        for h in range(1, EPG):
            ycopy(p, h).wait_recv()
        for c in range(0, width, 512):
            rows = stack([ybuf[p, h, :, c : c + 512] for h in range(EPG)])
            part = jnp.dot(mats, rows, preferred_element_type=F32)
            for half in range(2):
                both = part[half * group : (half + 1) * group] + part[(2 + half) * group : (3 + half) * group]
                s = 2 * p + half
                into = cbuf if s == HERE else cs
                into[s, :, c : c + 512] = both.astype(BF16)
        for half in range(2):
            if 2 * p + half != HERE:
                ccopy(2 * p + half).start()

    spread(0)
    for copy in loads[2:]:
        copy.wait()
    expert(0)
    spread(1)
    collect(0)
    expert(1)
    spread(2)
    spread(3)
    collect(1)
    expert(2)
    expert(3)
    collect(2)
    collect(3)

    lanes = lax.broadcasted_iota(jnp.int32, (tok, 128), 1)
    back = []
    for p in range(PAIRS):
        there = jnp.where(lanes < 64, lax.rem(z + HOPS[2 * p], planes), lax.rem(z + HOPS[2 * p + 1], planes))
        hit = (cols[:, 0:1] == there.astype(F32)) & (cols[:, 1:2] == (lanes & 63).astype(F32))
        back.append(jnp.where(hit, 1.0, 0.0))
    back = jnp.concatenate(back, axis=1).astype(BF16)
    for s in AWAY:
        ccopy(s).wait_recv()
    for c in range(0, width, 512):
        rows = stack([cbuf[s, :, c : c + 512] for s in range(planes)])
        part = jnp.dot(back, rows, preferred_element_type=F32)
        out_ref[:, c : c + 512] = (hidden[:, c : c + 512] + part).astype(BF16)

    for s in AWAY:
        mcopy(s).wait_send()
        zcopy(s).wait_send()
        ccopy(s).wait_send()
    for p in range(PAIRS):
        for h in range(1, EPG):
            xcopy(p, h).wait_send()
            ycopy(p, h).wait_send()


def layer_kernel(n_sp, n_tp, capacity, parts, *refs):
    cuts = [sum(parts[:i]) for i in range(len(parts) + 1)]
    mixed_in, later_in, out, joined, mixer_scratch, later_scratch = (
        refs[a:b] for a, b in zip(cuts, cuts[1:])
    )
    later = route_and_run(capacity, *joined, *later_in, *out, *later_scratch)
    drain = mix_heads(n_sp, n_tp, lambda: next(later), *mixed_in, *joined, *mixer_scratch)
    for _ in later:
        pass
    drain()


def layer(
    query_rows, key_rows, value_rows, forget_cum, doc_ids, residual, out_weight, norm_gain, expert_ids,
    route_weights, gate, up, down,
):
    n_sp, n_tp = lax.axis_size("sp"), lax.axis_size("tp")
    span, heads = query_rows.shape
    tok, width = residual.shape
    planes = n_sp // EPG
    capacity = max(2, 5 * tok // (4 * planes))
    group = 2 * capacity
    vmem = pl.BlockSpec(memory_space=pltpu.VMEM)
    hbm = pl.BlockSpec(memory_space=pl.ANY)
    dma = pltpu.SemaphoreType.DMA
    slots = pltpu.VMEM((planes, group, width), BF16)
    quads = pltpu.VMEM((PAIRS, EPG, group, width), BF16)
    mixer_scratch = [
        pltpu.VMEM((span, heads), BF16),
        pltpu.VMEM((span, heads), BF16),
        pltpu.VMEM((span, heads), BF16),
        pltpu.VMEM((8, span), F32),
        pltpu.VMEM((span, heads), BF16),
        pltpu.VMEM((span, heads), BF16),
        pltpu.VMEM((8, span), F32),
        pltpu.VMEM((REACH, span, heads), BF16),
        pltpu.VMEM((REACH, span, heads), BF16),
        pltpu.VMEM((REACH, 8, span), F32),
        pltpu.VMEM((2, span, 2 * heads), BF16),
        pltpu.VMEM((2 * heads, span), BF16),
        pltpu.VMEM((2, span, heads), BF16),
        pltpu.VMEM((2, span, 128), F32),
        pltpu.VMEM((2, span, 128), F32),
        pltpu.VMEM((span, heads), BF16),
        pltpu.VMEM((n_tp, tok, heads), BF16),
        dma((3,)),
        dma((1 + 2 * CUTS,)), dma((1 + 2 * CUTS,)), dma((1 + 2 * CUTS,)),
        dma((REACH, 1 + 2 * CUTS)), dma((REACH, 1 + 2 * CUTS)),
        dma((n_tp,)), dma((n_tp,)),
    ]
    later_scratch = [
        pltpu.VMEM((tok, width), BF16),
        pltpu.VMEM(out_weight.shape, BF16),
        pltpu.VMEM(gate.shape, BF16),
        pltpu.VMEM(up.shape, BF16),
        pltpu.VMEM(down.shape, BF16),
        pltpu.VMEM((tok, width), F32),
        pltpu.VMEM((tok, width), BF16),
        slots, slots,
        pltpu.VMEM((planes, 16, 128), BF16),
        pltpu.VMEM((planes, 16, 128), BF16),
        pltpu.VMEM((planes, group, 128), F32),
        quads, quads, quads, quads,
        slots, slots,
        dma((5,)),
        dma((planes,)), dma((planes,)), dma((planes,)), dma((planes,)),
        dma((PAIRS, EPG)), dma((PAIRS, EPG)), dma((PAIRS, EPG)), dma((PAIRS, EPG)),
        dma((planes,)), dma((planes,)),
    ]
    parts = (5, 8, 1, 1, len(mixer_scratch), len(later_scratch))
    return pl.pallas_call(
        functools.partial(layer_kernel, n_sp, n_tp, capacity, parts),
        out_shape=jax.ShapeDtypeStruct((tok, width), BF16),
        in_specs=[hbm] * 3 + [vmem] * 5 + [hbm] * 5,
        out_specs=vmem,
        scratch_shapes=[pltpu.VMEM((tok, heads * n_tp), BF16)] + mixer_scratch + later_scratch,
        compiler_params=pltpu.CompilerParams(
            collective_id=0, has_side_effects=True, vmem_limit_bytes=67043328
        ),
        name="layer",
    )(
        query_rows, key_rows, value_rows, forget_cum, doc_ids[None, :], norm_gain[None, :], expert_ids.T,
        route_weights.T, residual, out_weight, gate, up, down,
    )


def per_device(
    query_rows,
    key_rows,
    value_rows,
    forget_cum,
    doc_ids,
    residual,
    out_weight,
    norm_gain,
    expert_ids,
    route_weights,
    gate_proj,
    up_proj,
    down_proj,
):
    return layer(
        query_rows, key_rows, value_rows, forget_cum, doc_ids, residual, out_weight, norm_gain, expert_ids,
        route_weights, gate_proj[0], up_proj[0], down_proj[0],
    )


def solution(mesh):
    placed = (
        P("sp", "tp"),
        P("sp", "tp"),
        P("sp", "tp"),
        P("tp", "sp"),
        P("sp"),
        P(("sp", "tp"), None),
        P(),
        P(),
        P(("sp", "tp"), None),
        P(("sp", "tp"), None),
        P("sp", None, None),
        P("sp", None, None),
        P("sp", None, None),
    )
    return jax.shard_map(
        per_device, mesh=mesh, in_specs=placed, out_specs=P(("sp", "tp"), None), check_vma=False
    )
```
